32 devices in a mesh: vp: 4 (over y, x), dp: 8 (over z, core).
Axes of the slice: x: 2, y: 2, z: 4, core: 2. Of those that a mesh axis runs over, the one named last changes fastest.
Arguments:
- hidden_act: bfloat16 [4096, 8192], P('dp', 'vp'), may hold values from 0 to 36
- down_weight: bfloat16 [8192, 2048], P('vp'), may hold values from -0.0625 to 0.0625
- residual: bfloat16 [4096, 2048], P(('dp', 'vp')), may hold values from -300 to 300
- post_gain: float32 [2048], replicated, may hold values from 0.1 to 1.9
- final_gain: float32 [2048], replicated, may hold values from 0.1 to 1.9
- vocab: bfloat16 [2048, 32768], P(None, 'vp'), may hold values from -0.33 to 0.33
- vocab_bias: float32 [32768], P('vp'), may hold values from -2.5 to 2.5
- target_ids: int32 [4096, 4], P('dp'), may hold values from 0 to 32767
- target_weights: float32 [4096, 4], P('dp'), may hold values from 0 to 1, as said below
Outputs:
- losses: float32 [4096], P(('dp', 'vp'))
- stream_grad: float32 [4096, 2048], P(('dp', 'vp'))
- vocab_grad: float32 [2048, 32768], P('dp', 'vp')
The draws below stay inside these ranges and needn't reach their ends.
Inputs may be any that keep to these rules, and one draw needn't show every extreme that they name: `target_weights`: the 4 weights of a token add up to one.
All inputs are finite; a program needn't handle non-finite values.
Results may differ from the reference program's by a relative error of at most 0.01225.
Values may be sent and summed in bfloat16 or wider, within the bound.
A program may use at most 192 MiB of HBM per device.

```python
import math
import jax
import jax.numpy as jnp
import numpy as np
from jax import lax

D = 2048
FF = 8192
V = 32768
TOPK = 4
TOK_GRP = 512
TOKENS = 4096
N_VP = 4
N_DP = 8


def spike_signs(key):
    return (jax.random.randint(jax.random.fold_in(key, 4242), (D,), 0, 2) * 2 - 1).astype(jnp.float32)


def draw_hidden_act(key, part):
    values = jax.random.normal(jax.random.fold_in(key, 41), (TOKENS, FF), jnp.float32)
    values = jnp.clip(values, -6.0, 6.0)
    positive = jnp.maximum(values, 0.0)
    return (positive * positive).astype(jnp.bfloat16)


def draw_residual(key, part):
    values = jnp.clip(jax.random.normal(jax.random.fold_in(key, 11), (TOKENS, D), jnp.float32), -6.0, 6.0)
    marked = (jnp.arange(TOKENS) % 61 == 3)[:, None]
    values = jnp.where(marked, 300.0 * spike_signs(key)[None, :], values)
    return values.astype(jnp.bfloat16)


def draw_vocab(key, part):
    values = 0.055 * jnp.clip(jax.random.normal(jax.random.fold_in(key, 21), (D, V), jnp.float32), -6.0, 6.0)
    marked = (jnp.arange(V) % 509 == 7)[None, :]
    values = jnp.where(marked, 256.0 / D * spike_signs(key)[:, None], values)
    return values.astype(jnp.bfloat16)


def draw_vocab_bias(key, part):
    offsets = jax.random.uniform(jax.random.fold_in(key, 31), (N_VP,), jnp.float32, -1.5, 1.5)
    shard_of = jnp.arange(V) // (V // N_VP)
    values = 0.5 * jnp.clip(jax.random.normal(jax.random.fold_in(key, 32), (V,), jnp.float32), -2.0, 2.0)
    return offsets[shard_of] + values


def draw_target_weights(key, part):
    logits = 1.5 * jax.random.normal(jax.random.fold_in(key, 52), (TOKENS, TOPK), jnp.float32)
    return jax.nn.softmax(logits, axis=-1)


def place_ends(entries, key, smallest, top_value):
    spot = [jax.random.randint(jax.random.fold_in(key, axis), (), 0, length) for axis, length in enumerate(entries.shape)]
    widest = entries.shape.index(max(entries.shape))
    next_to = spot[:widest] + [(spot[widest] + 1) % entries.shape[widest]] + spot[widest + 1:]
    return entries.at[tuple(spot)].set(smallest).at[tuple(next_to)].set(top_value)


def steps_of(own_key, extent, cuts, low, largest):
    factor_of = 1.0
    for axis_at, parts in cuts:
        draws = jax.random.uniform(jax.random.fold_in(jax.random.fold_in(own_key, 6), axis_at), (parts,), jnp.float32, low / len(cuts), largest / len(cuts))
        factor_of = factor_of * jnp.repeat(jnp.exp(draws), extent[axis_at] // parts).reshape((-1,) + (1,) * (len(extent) - 1 - axis_at))
    return factor_of


def rank_table(amount, slope):
    weights = [(1 << 20) // math.isqrt(standing ** slope) + 1 for standing in range(1, amount + 1)]
    scale = 1 + sum(weights) // (1 << 30)
    return np.cumsum(np.array([max(1, weight // scale) for weight in weights]))


def ranked_ids(stream_key, shape, count, slope):
    table = rank_table(count, slope)
    pick = jax.random.randint(jax.random.fold_in(stream_key, 1), shape, 0, int(table[count - 1]))
    standing = jnp.searchsorted(jnp.asarray(table, jnp.int32), pick, side="right")
    return jax.random.permutation(jax.random.fold_in(stream_key, 2), count)[standing].astype(jnp.int32)


def centred(key, dims, scale, reach, pieces=(), kind=jnp.bfloat16):
    values = scale * jax.random.normal(key, dims, jnp.float32)
    if pieces:
        values = values * steps_of(key, dims, pieces, -0.22, 0.18)
    return jnp.clip(values, -reach, reach).astype(kind)


def setup_inputs(seed: int = 0) -> dict:
    splits = jax.random.split(jax.random.key(seed), 10)
    hidden_act = draw_hidden_act(jax.random.fold_in(splits[9], 71), 0)
    down_weight = centred(splits[1], (FF, D), FF ** -0.5, 0.0625, ((0, 4),))
    residual = draw_residual(jax.random.fold_in(splits[9], 71), 0)
    post_gain = jnp.clip(1.0 + 0.18 * jax.random.normal(splits[3], (D,), jnp.float32), 0.1, 1.9)
    final_gain = jnp.clip(1.0 + 0.18 * jax.random.normal(splits[4], (D,), jnp.float32), 0.1, 1.9)
    vocab = draw_vocab(jax.random.fold_in(splits[9], 71), 0)
    vocab_bias = draw_vocab_bias(jax.random.fold_in(splits[9], 71), 0)
    target_ids = place_ends(ranked_ids(splits[7], (TOKENS, TOPK), V, 2), jax.random.fold_in(splits[7], 3), 0, V - 1).astype(jnp.int32)
    target_weights = draw_target_weights(jax.random.fold_in(splits[9], 71), 0)
    return dict(hidden_act=hidden_act, down_weight=down_weight, residual=residual, post_gain=post_gain, final_gain=final_gain, vocab=vocab, vocab_bias=vocab_bias, target_ids=target_ids, target_weights=target_weights)


epsilon = 1e-06
z_weight = 0.001
loss_scale = 32.0

def inverse_rms(values):
    return lax.rsqrt(lax.optimization_barrier(jnp.mean(values * values, axis=-1, keepdims=True)) + epsilon)

def reference(hidden_act, down_weight, residual, post_gain, final_gain, vocab, vocab_bias, target_ids, target_weights):
    branch = jnp.dot(hidden_act, down_weight, preferred_element_type=jnp.float32)
    stream = residual.astype(jnp.float32) + branch * inverse_rms(branch) * post_gain
    inverse = inverse_rms(stream)
    normed = (stream * inverse * final_gain).astype(jnp.bfloat16)
    columns = jnp.arange(V, dtype=jnp.int32)[None, :]

    def group(matrix_acc, inputs):
        row_block, target_block, weight_block = inputs
        scores = jnp.dot(row_block, vocab, preferred_element_type=jnp.float32) + vocab_bias
        row_max = lax.optimization_barrier(jnp.max(scores, axis=1))
        row_sum = lax.optimization_barrier(jnp.sum(jnp.exp(scores - row_max[:, None]), axis=1))
        log_norm = row_max + jnp.log(row_sum)
        wanted = jnp.zeros(scores.shape, jnp.float32)
        for target_k in range(TOPK):
            wanted = wanted + jnp.where(target_block[:, target_k:target_k + 1] == columns, weight_block[:, target_k:target_k + 1], 0.0)
        target_score = lax.optimization_barrier(jnp.sum(wanted * scores, axis=1))
        losses = log_norm - target_score + z_weight * log_norm * log_norm
        probability = jnp.exp(scores - log_norm[:, None])
        score_grads = (loss_scale * (probability * (1.0 + 2.0 * z_weight * log_norm)[:, None] - wanted)).astype(jnp.bfloat16)
        row_grad = lax.dot_general(score_grads, vocab, (((1,), (1,)), ((), ())), preferred_element_type=jnp.float32)
        matrix_acc = matrix_acc + lax.dot_general(row_block, score_grads, (((0,), (0,)), ((), ())), preferred_element_type=jnp.float32)
        return (matrix_acc, (losses, row_grad))
    stacked = (normed.reshape(N_DP, TOK_GRP, D), target_ids.reshape(N_DP, TOK_GRP, TOPK), target_weights.reshape(N_DP, TOK_GRP, TOPK))
    vocab_grad, outputs = lax.scan(group, jnp.zeros((D, V), jnp.float32), stacked)
    losses = outputs[0].reshape(TOKENS)
    row_grad = outputs[1].reshape(TOKENS, D)
    upstream = row_grad * final_gain
    stream_grad = inverse * (upstream - stream * inverse * inverse * lax.optimization_barrier(jnp.mean(upstream * stream, axis=-1, keepdims=True)))
    return (losses, stream_grad, vocab_grad)
```

```python
import functools

import jax
import jax.numpy as jnp
from jax import lax
from jax.experimental import pallas as pl
from jax.experimental.pallas import tpu as pltpu
from jax.sharding import PartitionSpec as P

MESH = pl.DeviceIdType.MESH
CORES = 2
PLANE = 4
TILE = 512
CHUNKS = 4

epsilon = 1e-06
z_weight = 0.001
loss_scale = 32.0
f32 = jnp.float32
bf16 = jnp.bfloat16


def remote(src, dst, send_sem, recv_sem, vp, dp):
    return pltpu.make_async_remote_copy(
        src_ref=src,
        dst_ref=dst,
        send_sem=send_sem,
        recv_sem=recv_sem,
        device_id={"vp": vp, "dp": dp},
        device_id_type=MESH,
    )


class Place:
    def __init__(self, nz):
        self.nz = nz
        self.p = lax.axis_index("vp")
        self.dp = lax.axis_index("dp")
        self.z = self.dp // CORES
        self.c = lax.rem(self.dp, CORES)
        self.px = self.p + 1 - 2 * lax.rem(self.p, 2)
        self.py = lax.rem(self.p + 2, PLANE)
        self.pd = PLANE - 1 - self.p
        self.plane = (self.px, self.py, self.pd)

    def at(self, z):
        return z * CORES + self.c

    def ahead(self, k):
        return lax.rem(self.z + k, self.nz)

    def behind(self, k):
        return lax.rem(self.z - k + self.nz, self.nz)


def greet(peers):
    barrier = pltpu.get_barrier_semaphore()
    for vp, dp in peers:
        pl.semaphore_signal(barrier, inc=1, device_id={"vp": vp, "dp": dp}, device_id_type=MESH)
    pl.semaphore_wait(barrier, len(peers))


def rows_to_column(row):
    n = row.shape[1]
    eye = lax.broadcasted_iota(jnp.int32, (n, n), 0) == lax.broadcasted_iota(jnp.int32, (n, n), 1)
    return jnp.sum(jnp.where(eye, row, 0.0), axis=1, keepdims=True)


def column_to_row(column):
    n = column.shape[0]
    eye = lax.broadcasted_iota(jnp.int32, (n, n), 0) == lax.broadcasted_iota(jnp.int32, (n, n), 1)
    return jnp.sum(jnp.where(eye, column, 0.0), axis=0, keepdims=True)


def forward_kernel(
    nz,
    topk,
    hidden,
    down_hbm,
    resid,
    post_gain,
    final_gain,
    vocab_hbm,
    bias,
    target,
    normed_hbm,
    grads_hbm,
    stream_out,
    losses_out,
    down,
    vocab,
    partial,
    own,
    tosend,
    arrived,
    gathered,
    scores,
    targets,
    columns_of,
    lse_col,
    tgt_col,
    stat,
    stat_plane,
    stat_mid,
    stat_line,
    grads,
    down_sem,
    vocab_sem,
    tgt_send,
    tgt_recv,
    rs_send,
    rs_recv,
    ag_send,
    ag_recv,
    st_send,
    st_recv,
    out_sem,
    grads_sem,
):
    me = Place(nz)
    p, z, c = me.p, me.z, me.c
    rows, width = resid.shape
    group = hidden.shape[0]
    span = vocab.shape[1]
    tiles = width // TILE

    def down_copy(t):
        cut = pl.ds(pl.multiple_of(t * TILE, TILE), TILE)
        return pltpu.make_async_copy(down_hbm.at[:, cut], down.at[:, cut], down_sem.at[t])

    for t in range(tiles):
        down_copy(t).start()
    vocab_copy = pltpu.make_async_copy(
        vocab_hbm.at[:, pl.ds(pl.multiple_of(z * span, span), span)], vocab, vocab_sem
    )
    vocab_copy.start()

    line = [(p, me.at(me.ahead(k))) for k in range(1, nz)]
    greet([(q, me.dp) for q in me.plane] + line)

    def target_copy(k):
        return remote(target, targets.at[z], tgt_send.at[k - 1], tgt_recv.at[k - 1], p, me.at(me.ahead(k)))

    for k in range(1, nz):
        target_copy(k).start()
    targets[z] = target[...]

    def piece(kind, t):
        q = me.plane[kind]
        cut = pl.ds(pl.multiple_of(t * TILE, TILE), TILE)
        return remote(
            tosend.at[pl.ds(pl.multiple_of(q * rows, rows), rows), cut],
            arrived.at[kind, :, cut],
            rs_send.at[kind, t],
            rs_recv.at[kind, t],
            q,
            me.dp,
        )

    def down_tile(t, _):
        down_copy(t).wait()
        cut = pl.ds(pl.multiple_of(t * TILE, TILE), TILE)
        partial[...] = jnp.dot(hidden[...], down[:, cut], preferred_element_type=f32)
        tosend[:, cut] = partial[...].astype(bf16)
        own[:, cut] = partial[pl.ds(pl.multiple_of(p * rows, rows), rows), :]
        for kind in (2, 0, 1):
            piece(kind, t).start()
        return 0

    lax.fori_loop(0, tiles, down_tile, 0)
    for t in range(tiles):
        for kind in range(3):
            piece(kind, t).wait_recv()

    step = 16

    def norm_rows(i, _):
        r = pl.ds(pl.multiple_of(i * step, step), step)
        branch = own[r, :]
        for kind in range(3):
            branch = branch + arrived[kind, r, :].astype(f32)
        scale = lax.rsqrt(jnp.mean(branch * branch, axis=1, keepdims=True) + epsilon)
        stream = resid[r, :].astype(f32) + branch * scale * post_gain[...]
        inverse = lax.rsqrt(jnp.mean(stream * stream, axis=1, keepdims=True) + epsilon)
        stream_out[r, :] = stream
        gathered[z, pl.ds(pl.multiple_of(p * rows + i * step, step), step), :] = (
            stream * inverse * final_gain[...]
        ).astype(bf16)
        return 0

    lax.fori_loop(0, rows // step, norm_rows, 0)

    def block(zz, q):
        return gathered.at[zz, pl.ds(pl.multiple_of(q * rows, rows), rows), :]

    def send(zz, q, way, kind, vp, dp):
        return remote(block(zz, q), block(zz, q), ag_send.at[zz, way], ag_recv.at[zz, kind], vp, dp)

    def to_x(zz):
        return send(zz, p, 0, 1, me.px, me.dp)

    def to_y(zz):
        return send(zz, p, 1, 2, me.py, me.dp)

    def up(zz):
        return send(zz, p, 2, 0, p, me.dp + CORES)

    def below(zz):
        return send(zz, p, 3, 0, p, me.dp - CORES)

    def corner_y(zz):
        return send(zz, me.px, 4, 3, me.py, me.dp)

    def corner_x(zz):
        return send(zz, me.py, 4, 3, me.px, me.dp)

    def landed(zz, kind, q):
        return remote(block(zz, q), block(zz, q), ag_send.at[zz, 0], ag_recv.at[zz, kind], p, me.dp)

    def column_stage(s, zz):
        @pl.when(s > 0)
        def _():
            landed(zz, 0, p).wait_recv()

        @pl.when((zz <= z) & (z + 1 < nz))
        def _():
            up(zz).start()

        @pl.when((zz >= z) & (z > 0))
        def _():
            below(zz).start()

        to_x(zz).start()
        to_y(zz).start()

    def corner_stage(zz):
        landed(zz, 1, me.px).wait_recv()

        @pl.when(lax.rem(zz, 2) == 0)
        def _():
            corner_y(zz).start()

        landed(zz, 2, me.py).wait_recv()

        @pl.when(lax.rem(zz, 2) == 1)
        def _():
            corner_x(zz).start()

    first_column = p * vocab_hbm.shape[1] + z * span
    position = lax.broadcasted_iota(jnp.int32, (1, span), 1).astype(f32)
    chunk = 32
    lanes = 128

    def wanted_of(zz, r):
        total = None
        for k in range(topk):
            ids = columns_of[zz, r, k : k + 1] - first_column.astype(f32)
            weight = columns_of[zz, r, topk + k : topk + k + 1]
            term = jnp.where(ids == position, weight, 0.0)
            total = term if total is None else total + term
        return total

    row_at = lax.broadcasted_iota(jnp.int32, (2 * nz, lanes), 0)
    stat[...] = jnp.zeros_like(stat)

    def row_of(ref, q, cut):
        return jnp.sum(jnp.where(row_at == q, ref[:, cut], 0.0), axis=0, keepdims=True)

    def compute_stage(zz):
        landed(zz, 3, me.pd).wait_recv()

        def tile(t, _):
            cut = pl.ds(pl.multiple_of(t * TILE, TILE), TILE)
            at = pl.ds(pl.multiple_of(z * span + t * TILE, TILE), TILE)
            scores[zz, :, cut] = (
                jnp.dot(gathered[zz], vocab[:, cut], preferred_element_type=f32) + bias[:, at]
            )
            return 0

        lax.fori_loop(0, span // TILE, tile, 0)

        def stats(i, _):
            r = pl.ds(pl.multiple_of(i * chunk, chunk), chunk)
            values = scores[zz, r, :]
            largest = jnp.max(values, axis=1, keepdims=True)
            total = jnp.sum(jnp.exp(values - largest), axis=1, keepdims=True)
            lse_col[r, :] = largest + jnp.log(total)
            tgt_col[r, :] = jnp.sum(wanted_of(zz, r) * values, axis=1, keepdims=True)
            return 0

        lax.fori_loop(0, group // chunk, stats, 0)
        for j in range(group // lanes):
            cut = slice(j * lanes, (j + 1) * lanes)
            kept = jnp.where(row_at == zz, column_to_row(lse_col[cut, :]), stat[:, cut])
            stat[:, cut] = jnp.where(row_at == nz + zz, column_to_row(tgt_col[cut, :]), kept)

    steps = 2 * nz - 1
    lag = 2

    def gather_step(i, _):
        def staged(s, stage):
            half = (s + 1) // 2
            zz = z + half * (1 - 2 * lax.rem(s, 2))

            @pl.when((zz >= 0) & (zz < nz))
            def _():
                stage(zz)

        @pl.when(i < steps)
        def _():
            staged(i, functools.partial(column_stage, i))

        @pl.when((i >= lag) & (i < steps + lag))
        def _():
            staged(i - lag, corner_stage)

        @pl.when(i == 2 * lag)
        def _():
            vocab_copy.wait()
            for k in range(1, nz):
                zk = me.behind(k)
                remote(
                    target, targets.at[zk], tgt_send.at[k - 1], tgt_recv.at[k - 1], p, me.at(zk)
                ).wait_recv()
            for q in range(nz):
                for j in range(group // lanes):
                    cut = slice(j * lanes, (j + 1) * lanes)
                    for k in range(2 * topk):
                        columns_of[q, cut, k : k + 1] = rows_to_column(targets[q, k : k + 1, cut])

        @pl.when(i >= 2 * lag)
        def _():
            staged(i - 2 * lag, compute_stage)

        return 0

    lax.fori_loop(0, steps + 2 * lag, gather_step, 0)
    normed_copy = pltpu.make_async_copy(gathered, normed_hbm, out_sem)
    normed_copy.start()

    def plane_stat(kind):
        return remote(stat, stat_plane.at[kind], st_send.at[kind], st_recv.at[kind], me.plane[kind], me.dp)

    for kind in range(3):
        plane_stat(kind).start()

    def combined(mine, others):
        lse = [mine[:nz]] + [o[:nz] for o in others]
        top = functools.reduce(jnp.maximum, lse)
        total = sum(jnp.exp(v - top) for v in lse)
        return top + jnp.log(total), mine[nz:] + sum(o[nz:] for o in others)

    for kind in range(3):
        plane_stat(kind).wait_recv()
    lse, tgt = combined(stat[...], [stat_plane[kind] for kind in range(3)])
    stat_mid[0:nz] = lse
    stat_mid[nz : 2 * nz] = tgt

    def line_stat(k):
        return remote(
            stat_mid, stat_line.at[k - 1], st_send.at[2 + k], st_recv.at[2 + k], p, me.at(me.ahead(k))
        )

    for k in range(1, nz):
        line_stat(k).start()
    for k in range(1, nz):
        line_stat(k).wait_recv()
    lse, tgt = combined(stat_mid[...], [stat_line[k] for k in range(nz - 1)])
    for kind in range(3):
        plane_stat(kind).wait_send()
    stat[0:nz] = lse
    stat[nz : 2 * nz] = tgt
    mine = pl.ds(pl.multiple_of(p * rows, rows), rows)
    own_at = lax.broadcasted_iota(jnp.int32, (2 * nz, rows), 0)
    own_lse = jnp.sum(jnp.where(own_at == z, stat[:, mine], 0.0), axis=0, keepdims=True)
    own_tgt = jnp.sum(jnp.where(own_at == nz + z, stat[:, mine], 0.0), axis=0, keepdims=True)
    losses_out[...] = own_lse - own_tgt + z_weight * own_lse * own_lse

    def grads_copy(q):
        return pltpu.make_async_copy(grads.at[lax.rem(q, 2)], grads_hbm.at[q], grads_sem.at[lax.rem(q, 2)])

    def grads_plane(q, _):
        @pl.when(q >= 2)
        def _():
            grads_copy(q - 2).wait()

        for j in range(group // lanes):
            cut = slice(j * lanes, (j + 1) * lanes)
            lse_col[cut, :] = rows_to_column(row_of(stat, q, cut))

        def some(i, _):
            r = pl.ds(pl.multiple_of(i * chunk, chunk), chunk)
            norm = lse_col[r, :]
            factor = loss_scale * (1.0 + 2.0 * z_weight * norm)
            grads[lax.rem(q, 2), r, :] = (
                jnp.exp(scores[q, r, :] - norm) * factor - loss_scale * wanted_of(q, r)
            ).astype(bf16)
            return 0

        lax.fori_loop(0, group // chunk, some, 0)
        grads_copy(q).start()
        return 0

    lax.fori_loop(0, nz, grads_plane, 0)
    for q in range(max(nz - 2, 0), nz):
        grads_copy(q).wait()
    normed_copy.wait()

    for k in range(1, nz):
        target_copy(k).wait_send()
        line_stat(k).wait_send()
    for t in range(tiles):
        for kind in range(3):
            piece(kind, t).wait_send()
    for zz in range(nz):
        to_x(zz).wait_send()
        to_y(zz).wait_send()
        corner_y(zz).wait_send()

        @pl.when((zz <= z) & (z + 1 < nz))
        def _():
            up(zz).wait_send()

        @pl.when((zz >= z) & (z > 0))
        def _():
            below(zz).wait_send()


def backward_kernel(
    nz,
    normed_hbm,
    grads_hbm,
    vocab_hbm,
    stream,
    final_gain,
    vgrad_hbm,
    sgrad_out,
    normed,
    grads,
    vocab,
    turned,
    block,
    core_send_buf,
    core_recv_buf,
    far_send_buf,
    far_recv_buf,
    part,
    first,
    second,
    line_recv_buf,
    total,
    in_sem,
    core_send,
    core_recv,
    far_send,
    far_recv,
    hop_send,
    hop_recv,
    line_send,
    line_recv,
    out_sem,
):
    me = Place(nz)
    p, z, c = me.p, me.z, me.c
    rows, width = stream.shape
    group = grads.shape[1]
    tokens = nz * group
    span = vocab.shape[1]
    deep = width // (nz * CORES)

    loads = [
        pltpu.make_async_copy(normed_hbm, normed, in_sem.at[0]),
        pltpu.make_async_copy(grads_hbm, grads, in_sem.at[1]),
        pltpu.make_async_copy(
            vocab_hbm.at[:, pl.ds(pl.multiple_of(z * span, span), span)], vocab, in_sem.at[2]
        ),
    ]
    for load in loads:
        load.start()

    partner = me.dp + 1 - 2 * c
    greet(
        [(p, partner), (me.px, me.dp), (me.py, me.dp)] + [(p, me.at(me.ahead(k))) for k in range(1, nz)]
    )
    loads[0].wait()
    loads[1].wait()

    def core_copy(i):
        return remote(
            core_send_buf.at[lax.rem(i, 2)], core_recv_buf.at[i], core_send.at[i], core_recv.at[i], p, partner
        )

    def far_copy(k, zk):
        return remote(
            far_send_buf.at[k - 1], far_recv_buf.at[z], far_send.at[k - 1], far_recv.at[k - 1], p, me.at(zk)
        )

    def product(dest, store):
        at = pl.ds(pl.multiple_of(dest * deep, deep), deep)
        for q in range(nz):
            turned[:, q * group : (q + 1) * group] = normed[q, :, at].T

        def tile(t, _):
            cut = pl.ds(pl.multiple_of(t * TILE, TILE), TILE)
            store(
                cut,
                jnp.dot(
                    turned[...], grads[:, :, cut].reshape(tokens, TILE), preferred_element_type=f32
                ),
            )
            return 0

        lax.fori_loop(0, span // TILE, tile, 0)

    def vocab_step(i, _):
        k = i + 1
        zk = me.ahead(k)

        @pl.when(i >= 2)
        def _():
            core_copy(i - 2).wait_send()

        def to_core(cut, value):
            core_send_buf[lax.rem(i, 2), :, cut] = value.astype(bf16)

        product(zk * CORES + 1 - c, to_core)
        core_copy(i).start()

        def to_block(cut, value):
            block[:, cut] = value

        product(me.at(zk), to_block)
        core_copy(i).wait_recv()

        def add(j, _):
            r = pl.ds(pl.multiple_of(j * 32, 32), 32)
            value = (block[r, :] + core_recv_buf[i, r, :].astype(f32)).astype(bf16)

            @pl.when(k < nz)
            def _():
                far_send_buf[k - 1, r, :] = value

            @pl.when(k == nz)
            def _():
                far_recv_buf[z, r, :] = value

            return 0

        lax.fori_loop(0, deep // 32, add, 0)

        @pl.when(k < nz)
        def _():
            far_copy(k, zk).start()

        return 0

    lax.fori_loop(0, nz, vocab_step, 0)
    loads[2].wait()

    def at_block(q):
        return pl.ds(pl.multiple_of(q * rows, rows), rows)

    def hop(zz, slot):
        near, target = (me.px, me.px) if zz % 2 == 0 else (me.py, me.py)
        q = near if slot == 0 else me.pd
        return remote(
            part.at[zz, at_block(q), :],
            first.at[zz, slot],
            hop_send.at[zz, slot],
            hop_recv.at[zz, slot],
            target,
            me.dp,
        )

    def turn(zz):
        target = me.py if zz % 2 == 0 else me.px
        return remote(part.at[zz, at_block(target), :], second.at[zz], hop_send.at[zz, 2], hop_recv.at[zz, 2], target, me.dp)

    def line_up(zz):
        return remote(
            part.at[zz, at_block(p), :], line_recv_buf.at[zz, 0], line_send.at[zz], line_recv.at[zz, 0], p, me.dp + CORES
        )

    def line_down(zz):
        return remote(
            part.at[zz, at_block(p), :], line_recv_buf.at[zz, 1], line_send.at[zz], line_recv.at[zz, 1], p, me.dp - CORES
        )

    step = 16
    pieces = rows // step

    def matmul_stage(zz):
        def tile(t, _):
            cut = pl.ds(pl.multiple_of(t * TILE, TILE), TILE)
            part[zz, :, cut] = lax.dot_general(
                grads[zz], vocab[cut, :], (((1,), (1,)), ((), ())), preferred_element_type=f32
            ).astype(bf16)
            return 0

        lax.fori_loop(0, width // TILE, tile, 0)
        hop(zz, 1).start()
        hop(zz, 0).start()

    def turn_stage(zz):
        hop(zz, 1).wait_recv()
        q = me.py if zz % 2 == 0 else me.px

        def some(i, _):
            r = pl.ds(pl.multiple_of(i * step, step), step)
            at = pl.ds(pl.multiple_of(q * rows + i * step, step), step)
            part[zz, at, :] = (part[zz, at, :].astype(f32) + first[zz, 1, r, :].astype(f32)).astype(bf16)
            return 0

        lax.fori_loop(0, pieces, some, 0)
        turn(zz).start()

    def line_stage(zz):
        hop(zz, 0).wait_recv()
        turn(zz).wait_recv()

        @pl.when((zz >= z) & (z > 0))
        def _():
            line_up(zz).wait_recv()

        @pl.when((zz <= z) & (z + 1 < nz))
        def _():
            line_down(zz).wait_recv()

        def some(i, _):
            r = pl.ds(pl.multiple_of(i * step, step), step)
            at = pl.ds(pl.multiple_of(p * rows + i * step, step), step)
            value = (
                part[zz, at, :].astype(f32) + first[zz, 0, r, :].astype(f32) + second[zz, r, :].astype(f32)
            )
            total[r, :] = value

            @pl.when((zz >= z) & (z > 0))
            def _():
                total[r, :] = total[r, :] + line_recv_buf[zz, 0, r, :].astype(f32)

            @pl.when((zz <= z) & (z + 1 < nz))
            def _():
                total[r, :] = total[r, :] + line_recv_buf[zz, 1, r, :].astype(f32)

            @pl.when(zz != z)
            def _():
                part[zz, at, :] = total[r, :].astype(bf16)

            @pl.when(zz == z)
            def _():
                rows_of = stream[r, :]
                inverse = lax.rsqrt(jnp.mean(rows_of * rows_of, axis=1, keepdims=True) + epsilon)
                upstream = total[r, :] * final_gain[...]
                sgrad_out[r, :] = inverse * (
                    upstream
                    - rows_of * inverse * inverse * jnp.mean(upstream * rows_of, axis=1, keepdims=True)
                )

            return 0

        lax.fori_loop(0, pieces, some, 0)

        @pl.when(zz > z)
        def _():
            line_up(zz).start()

        @pl.when(zz < z)
        def _():
            line_down(zz).start()

    order = []
    low, high = 0, nz - 1
    while low <= high:
        order.append(high)
        if low < high:
            order.append(low)
        low, high = low + 1, high - 1
    for i in range(nz + 2):
        if i < nz:
            matmul_stage(order[i])
        if 1 <= i <= nz:
            turn_stage(order[i - 1])
        if 2 <= i:
            line_stage(order[i - 2])

    def out_copy(q):
        return pltpu.make_async_copy(
            far_recv_buf.at[q], vgrad_hbm.at[:, pl.ds(pl.multiple_of(q * span, span), span)], out_sem.at[q]
        )

    out_copy(z).start()
    for k in range(1, nz):
        zk = me.behind(k)
        remote(
            far_send_buf.at[k - 1], far_recv_buf.at[zk], far_send.at[k - 1], far_recv.at[k - 1], p, me.at(zk)
        ).wait_recv()
        out_copy(zk).start()
    for q in range(nz):
        out_copy(q).wait()

    for k in range(1, nz):
        far_copy(k, me.ahead(k)).wait_send()
    for i in range(max(nz - 2, 0), nz):
        core_copy(i).wait_send()
    for zz in range(nz):
        hop(zz, 0).wait_send()
        hop(zz, 1).wait_send()
        turn(zz).wait_send()

        @pl.when(zz != z)
        def _():
            line_up(zz).wait_send()


def vmem():
    return pl.BlockSpec(memory_space=pltpu.VMEM)


def anywhere():
    return pl.BlockSpec(memory_space=pl.ANY)


def fast_shards(
    nz, hidden_act, down_weight, residual, post_gain, final_gain, vocab, vocab_bias, target_ids, target_weights
):
    rows, width = residual.shape
    group, hidden_units = hidden_act.shape
    columns = vocab.shape[1]
    span = columns // nz
    topk = target_ids.shape[1]
    tiles = width // TILE
    deep = width // (nz * CORES)
    dma = pltpu.SemaphoreType.DMA
    target = jnp.concatenate([target_ids.astype(f32), target_weights], axis=1).T
    normed, grads, stream, losses = pl.pallas_call(
        functools.partial(forward_kernel, nz, topk),
        name="forward",
        out_shape=(
            jax.ShapeDtypeStruct((nz, group, width), bf16),
            jax.ShapeDtypeStruct((nz, group, span), bf16),
            jax.ShapeDtypeStruct((rows, width), f32),
            jax.ShapeDtypeStruct((1, rows), f32),
        ),
        in_specs=[vmem(), anywhere(), vmem(), vmem(), vmem(), anywhere(), vmem(), vmem()],
        out_specs=(anywhere(), anywhere(), vmem(), vmem()),
        scratch_shapes=[
            pltpu.VMEM((hidden_units, width), bf16),
            pltpu.VMEM((width, span), bf16),
            pltpu.VMEM((group, TILE), f32),
            pltpu.VMEM((rows, width), f32),
            pltpu.VMEM((group, width), bf16),
            pltpu.VMEM((3, rows, width), bf16),
            pltpu.VMEM((nz, group, width), bf16),
            pltpu.VMEM((nz, group, span), f32),
            pltpu.VMEM((nz, 2 * topk, group), f32),
            pltpu.VMEM((nz, group, 2 * topk), f32),
            pltpu.VMEM((group, 1), f32),
            pltpu.VMEM((group, 1), f32),
            pltpu.VMEM((2 * nz, group), f32),
            pltpu.VMEM((3, 2 * nz, group), f32),
            pltpu.VMEM((2 * nz, group), f32),
            pltpu.VMEM((nz - 1, 2 * nz, group), f32),
            pltpu.VMEM((2, group, span), bf16),
            dma((tiles,)),
            dma,
            dma((nz - 1,)),
            dma((nz - 1,)),
            dma((3, tiles)),
            dma((3, tiles)),
            dma((nz, 5)),
            dma((nz, 4)),
            dma((nz + 2,)),
            dma((nz + 2,)),
            dma,
            dma((2,)),
        ],
        compiler_params=pltpu.CompilerParams(
            collective_id=0, has_side_effects=True, vmem_limit_bytes=66 * 1000 * 1000
        ),
    )(
        hidden_act,
        down_weight,
        residual,
        post_gain[None, :],
        final_gain[None, :],
        vocab,
        vocab_bias[None, :],
        target,
    )
    vocab_grad, stream_grad = pl.pallas_call(
        functools.partial(backward_kernel, nz),
        name="backward",
        out_shape=(
            jax.ShapeDtypeStruct((deep, columns), bf16),
            jax.ShapeDtypeStruct((rows, width), f32),
        ),
        in_specs=[anywhere(), anywhere(), anywhere(), vmem(), vmem()],
        out_specs=(anywhere(), vmem()),
        scratch_shapes=[
            pltpu.VMEM((nz, group, width), bf16),
            pltpu.VMEM((nz, group, span), bf16),
            pltpu.VMEM((width, span), bf16),
            pltpu.VMEM((deep, nz * group), bf16),
            pltpu.VMEM((deep, span), f32),
            pltpu.VMEM((2, deep, span), bf16),
            pltpu.VMEM((nz, deep, span), bf16),
            pltpu.VMEM((nz - 1, deep, span), bf16),
            pltpu.VMEM((nz, deep, span), bf16),
            pltpu.VMEM((nz, group, width), bf16),
            pltpu.VMEM((nz, 2, rows, width), bf16),
            pltpu.VMEM((nz, rows, width), bf16),
            pltpu.VMEM((nz, 2, rows, width), bf16),
            pltpu.VMEM((rows, width), f32),
            dma((3,)),
            dma((nz,)),
            dma((nz,)),
            dma((nz - 1,)),
            dma((nz - 1,)),
            dma((nz, 3)),
            dma((nz, 3)),
            dma((nz,)),
            dma((nz, 2)),
            dma((nz,)),
        ],
        compiler_params=pltpu.CompilerParams(
            collective_id=1, has_side_effects=True, vmem_limit_bytes=66 * 1000 * 1000
        ),
    )(normed, grads, vocab, stream, final_gain[None, :])
    return losses[0], stream_grad, vocab_grad.astype(f32)


def inverse_rms(values):
    return lax.rsqrt(jnp.mean(values * values, axis=-1, keepdims=True) + epsilon)


def general_shards(
    hidden_act,
    down_weight,
    residual,
    post_gain,
    final_gain,
    vocab,
    vocab_bias,
    target_ids,
    target_weights,
):
    own_rows = residual.shape[0]
    group_rows = hidden_act.shape[0]
    columns = vocab.shape[1]
    vp_index = lax.axis_index("vp")
    branch = lax.psum_scatter(
        jnp.dot(hidden_act, down_weight, preferred_element_type=jnp.float32),
        "vp",
        scatter_dimension=0,
        tiled=True,
    )
    stream = residual.astype(jnp.float32) + branch * inverse_rms(branch) * post_gain
    inverse = inverse_rms(stream)
    normed = (stream * inverse * final_gain).astype(jnp.bfloat16)
    gathered = lax.all_gather(normed, "vp", axis=0, tiled=True)
    local_ids = target_ids - vp_index * columns
    position = lax.broadcasted_iota(jnp.int32, (1, columns), 1)
    wanted = jnp.zeros((group_rows, columns), jnp.float32)
    for target_k in range(target_ids.shape[1]):
        wanted = wanted + jnp.where(
            local_ids[:, target_k : target_k + 1] == position,
            target_weights[:, target_k : target_k + 1],
            0.0,
        )
    scores = jnp.dot(gathered, vocab, preferred_element_type=jnp.float32) + vocab_bias[None, :]
    local_max = jnp.max(scores, axis=1)
    local_sum = jnp.sum(jnp.exp(scores - local_max[:, None]), axis=1)
    local_target = jnp.sum(wanted * scores, axis=1)
    stats = lax.all_gather(jnp.stack([local_max, local_sum, local_target]), "vp", axis=0)
    row_max = jnp.max(stats[:, 0], axis=0)
    row_sum = jnp.sum(stats[:, 1] * jnp.exp(stats[:, 0] - row_max), axis=0)
    target_score = jnp.sum(stats[:, 2], axis=0)
    log_norm = row_max + jnp.log(row_sum)
    group_losses = log_norm - target_score + z_weight * log_norm * log_norm
    losses = lax.dynamic_slice_in_dim(group_losses, vp_index * own_rows, own_rows, 0)
    factor = (1.0 + 2.0 * z_weight * log_norm)[:, None]
    probability = jnp.exp(scores - log_norm[:, None])
    score_grads = (loss_scale * (probability * factor - wanted)).astype(jnp.bfloat16)
    chunk = columns // CHUNKS
    pieces = []
    for index in range(CHUNKS):
        part = score_grads[:, index * chunk : (index + 1) * chunk]
        grad = lax.dot_general(
            gathered, part, (((0,), (0,)), ((), ())), preferred_element_type=jnp.float32
        ).astype(jnp.bfloat16)
        pieces.append(lax.psum_scatter(grad, "dp", scatter_dimension=0, tiled=True))
    row_grad = lax.psum_scatter(
        lax.dot_general(
            score_grads, vocab, (((1,), (1,)), ((), ())), preferred_element_type=jnp.float32
        ),
        "vp",
        scatter_dimension=0,
        tiled=True,
    )
    vocab_grad = jnp.concatenate([piece.astype(jnp.float32) for piece in pieces], axis=1)
    upstream = row_grad * final_gain
    stream_grad = inverse * (
        upstream - stream * inverse * inverse * jnp.mean(upstream * stream, axis=-1, keepdims=True)
    )
    return (losses, stream_grad, vocab_grad)


def solution(mesh):
    in_specs = (
        P("dp", "vp"),
        P("vp", None),
        P(("dp", "vp"), None),
        P(),
        P(),
        P(None, "vp"),
        P("vp"),
        P("dp", None),
        P("dp", None),
    )
    out_specs = (P(("dp", "vp")), P(("dp", "vp"), None), P("dp", "vp"))
    body = general_shards
    if mesh.shape["vp"] == PLANE and mesh.shape["dp"] % CORES == 0:
        body = functools.partial(fast_shards, mesh.shape["dp"] // CORES)
    return jax.shard_map(body, mesh=mesh, in_specs=in_specs, out_specs=out_specs, check_vma=False)
```

```python
import functools

import jax
import jax.numpy as jnp
from jax import lax
from jax.experimental import pallas as pl
from jax.experimental.pallas import tpu as pltpu
from jax.sharding import PartitionSpec as P

MESH = pl.DeviceIdType.MESH
CORES = 2
PLANE = 4
LINE = 4
TILE = 512
CHUNKS = 4

epsilon = 1e-06
z_weight = 0.001
loss_scale = 32.0
f32 = jnp.float32
bf16 = jnp.bfloat16


def remote(src, dst, send_sem, recv_sem, vp, dp):
    return pltpu.make_async_remote_copy(
        src_ref=src,
        dst_ref=dst,
        send_sem=send_sem,
        recv_sem=recv_sem,
        device_id={"vp": vp, "dp": dp},
        device_id_type=MESH,
    )


class Place:
    def __init__(self, nz):
        self.nz = nz
        self.p = lax.axis_index("vp")
        self.dp = lax.axis_index("dp")
        self.z = self.dp // CORES
        self.c = lax.rem(self.dp, CORES)
        self.px = self.p + 1 - 2 * lax.rem(self.p, 2)
        self.py = lax.rem(self.p + 2, PLANE)
        self.pd = PLANE - 1 - self.p
        self.plane = (self.px, self.py, self.pd)

    def at(self, z):
        return z * CORES + self.c

    def ahead(self, k):
        return lax.rem(self.z + k, self.nz)

    def behind(self, k):
        return lax.rem(self.z - k + self.nz, self.nz)


def greet(peers):
    barrier = pltpu.get_barrier_semaphore()
    for vp, dp in peers:
        pl.semaphore_signal(barrier, inc=1, device_id={"vp": vp, "dp": dp}, device_id_type=MESH)
    pl.semaphore_wait(barrier, len(peers))


def rows_to_column(row):
    n = row.shape[1]
    eye = lax.broadcasted_iota(jnp.int32, (n, n), 0) == lax.broadcasted_iota(jnp.int32, (n, n), 1)
    return jnp.sum(jnp.where(eye, row, 0.0), axis=1, keepdims=True)


def column_to_row(column):
    n = column.shape[0]
    eye = lax.broadcasted_iota(jnp.int32, (n, n), 0) == lax.broadcasted_iota(jnp.int32, (n, n), 1)
    return jnp.sum(jnp.where(eye, column, 0.0), axis=0, keepdims=True)


def forward_kernel(
    nz,
    topk,
    hidden,
    down_hbm,
    resid,
    post_gain,
    final_gain,
    vocab_hbm,
    bias,
    target,
    normed_hbm,
    grads_hbm,
    stream_out,
    losses_out,
    down,
    vocab,
    partial,
    own,
    tosend,
    arrived,
    gathered,
    scores,
    targets,
    columns_of,
    lse_col,
    tgt_col,
    stat,
    stat_plane,
    stat_mid,
    stat_line,
    grads,
    down_sem,
    vocab_sem,
    tgt_send,
    tgt_recv,
    rs_send,
    rs_recv,
    ag_send,
    ag_recv,
    st_send,
    st_recv,
    out_sem,
    grads_sem,
):
    me = Place(nz)
    p, z, c = me.p, me.z, me.c
    rows, width = resid.shape
    group = hidden.shape[0]
    span = vocab.shape[1]
    tiles = width // TILE

    def down_copy(t):
        cut = pl.ds(pl.multiple_of(t * TILE, TILE), TILE)
        return pltpu.make_async_copy(down_hbm.at[:, cut], down.at[:, cut], down_sem.at[t])

    for t in range(tiles):
        down_copy(t).start()
    vocab_copy = pltpu.make_async_copy(
        vocab_hbm.at[:, pl.ds(pl.multiple_of(z * span, span), span)], vocab, vocab_sem
    )
    vocab_copy.start()

    line = [(p, me.at(me.ahead(k))) for k in range(1, nz)]
    greet([(q, me.dp) for q in me.plane] + line)

    def target_copy(k):
        return remote(target, targets.at[z], tgt_send.at[k - 1], tgt_recv.at[k - 1], p, me.at(me.ahead(k)))

    for k in range(1, nz):
        target_copy(k).start()
    targets[z] = target[...]

    def piece(kind, t):
        q = me.plane[kind]
        cut = pl.ds(pl.multiple_of(t * TILE, TILE), TILE)
        return remote(
            tosend.at[pl.ds(pl.multiple_of(q * rows, rows), rows), cut],
            arrived.at[kind, :, cut],
            rs_send.at[kind, t],
            rs_recv.at[kind, t],
            q,
            me.dp,
        )

    def down_tile(t, _):
        down_copy(t).wait()
        cut = pl.ds(pl.multiple_of(t * TILE, TILE), TILE)
        partial[...] = jnp.dot(hidden[...], down[:, cut], preferred_element_type=f32)
        tosend[:, cut] = partial[...].astype(bf16)
        own[:, cut] = partial[pl.ds(pl.multiple_of(p * rows, rows), rows), :]
        for kind in (2, 0, 1):
            piece(kind, t).start()
        return 0

    lax.fori_loop(0, tiles, down_tile, 0)
    for t in range(tiles):
        for kind in range(3):
            piece(kind, t).wait_recv()

    step = 16

    def norm_rows(i, _):
        r = pl.ds(pl.multiple_of(i * step, step), step)
        branch = own[r, :]
        for kind in range(3):
            branch = branch + arrived[kind, r, :].astype(f32)
        scale = lax.rsqrt(jnp.mean(branch * branch, axis=1, keepdims=True) + epsilon)
        stream = resid[r, :].astype(f32) + branch * scale * post_gain[...]
        inverse = lax.rsqrt(jnp.mean(stream * stream, axis=1, keepdims=True) + epsilon)
        stream_out[r, :] = stream
        gathered[z, pl.ds(pl.multiple_of(p * rows + i * step, step), step), :] = (
            stream * inverse * final_gain[...]
        ).astype(bf16)
        return 0

    lax.fori_loop(0, rows // step, norm_rows, 0)

    def block(zz, q):
        return gathered.at[zz, pl.ds(pl.multiple_of(q * rows, rows), rows), :]

    def send(zz, q, way, kind, vp, dp):
        return remote(block(zz, q), block(zz, q), ag_send.at[zz, way], ag_recv.at[zz, kind], vp, dp)

    def to_x(zz):
        return send(zz, p, 0, 1, me.px, me.dp)

    def to_y(zz):
        return send(zz, p, 1, 2, me.py, me.dp)

    def up(zz):
        return send(zz, p, 2, 0, p, me.dp + CORES)

    def below(zz):
        return send(zz, p, 3, 0, p, me.dp - CORES)

    def corner_y(zz):
        return send(zz, me.px, 4, 3, me.py, me.dp)

    def corner_x(zz):
        return send(zz, me.py, 4, 3, me.px, me.dp)

    def landed(zz, kind, q):
        return remote(block(zz, q), block(zz, q), ag_send.at[zz, 0], ag_recv.at[zz, kind], p, me.dp)

    def column_stage(s, zz):
        @pl.when(s > 0)
        def _():
            landed(zz, 0, p).wait_recv()

        @pl.when((zz <= z) & (z + 1 < nz))
        def _():
            up(zz).start()

        @pl.when((zz >= z) & (z > 0))
        def _():
            below(zz).start()

        to_x(zz).start()
        to_y(zz).start()

    def corner_stage(zz):
        landed(zz, 1, me.px).wait_recv()

        @pl.when(lax.rem(zz, 2) == 0)
        def _():
            corner_y(zz).start()

        landed(zz, 2, me.py).wait_recv()

        @pl.when(lax.rem(zz, 2) == 1)
        def _():
            corner_x(zz).start()

    first_column = p * vocab_hbm.shape[1] + z * span
    position = lax.broadcasted_iota(jnp.int32, (1, span), 1).astype(f32)
    chunk = 32
    lanes = 128

    def wanted_of(zz, r):
        total = 0.0
        for k in range(topk):
            ids = columns_of[zz, r, k : k + 1] - first_column.astype(f32)
            total = jnp.where(ids == position, columns_of[zz, r, topk + k : topk + k + 1], total)
        return total

    row_at = lax.broadcasted_iota(jnp.int32, (2 * nz, lanes), 0)
    stat[...] = jnp.zeros_like(stat)

    def row_of(ref, q, cut):
        return jnp.sum(jnp.where(row_at == q, ref[:, cut], 0.0), axis=0, keepdims=True)

    pair = 2 * rows

    def compute_pair(zz, which):
        base = which * pair

        def tile(t, _):
            cut = pl.ds(pl.multiple_of(t * TILE, TILE), TILE)
            at = pl.ds(pl.multiple_of(z * span + t * TILE, TILE), TILE)
            r = pl.ds(pl.multiple_of(base, pair), pair)
            scores[zz, r, cut] = (
                jnp.dot(gathered[zz, r, :], vocab[:, cut], preferred_element_type=f32) + bias[:, at]
            )
            return 0

        lax.fori_loop(0, span // TILE, tile, 0)

        def stats(i, _):
            r = pl.ds(pl.multiple_of(base + i * chunk, chunk), chunk)
            at = pl.ds(pl.multiple_of(i * chunk, chunk), chunk)
            values = scores[zz, r, :]
            largest = jnp.max(values, axis=1, keepdims=True)
            total = jnp.sum(jnp.exp(values - largest), axis=1, keepdims=True)
            lse_col[at, :] = largest + jnp.log(total)
            tgt_col[at, :] = jnp.sum(wanted_of(zz, r) * values, axis=1, keepdims=True)
            return 0

        lax.fori_loop(0, pair // chunk, stats, 0)
        for j in range(pair // lanes):
            cut = slice(j * lanes, (j + 1) * lanes)
            at = pl.ds(pl.multiple_of(base + j * lanes, lanes), lanes)
            kept = jnp.where(row_at == zz, column_to_row(lse_col[cut, :]), stat[:, at])
            stat[:, at] = jnp.where(row_at == nz + zz, column_to_row(tgt_col[cut, :]), kept)

    def compute_stage(zz):
        compute_pair(zz, p // 2)
        landed(zz, 3, me.pd).wait_recv()
        compute_pair(zz, 1 - p // 2)

    steps = 2 * nz - 1
    lag = 2

    def gather_step(i, _):
        def staged(s, stage):
            half = (s + 1) // 2
            zz = z + half * (1 - 2 * lax.rem(s, 2))

            @pl.when((zz >= 0) & (zz < nz))
            def _():
                stage(zz)

        @pl.when(i < steps)
        def _():
            staged(i, functools.partial(column_stage, i))

        @pl.when((i >= lag) & (i < steps + lag))
        def _():
            staged(i - lag, corner_stage)

        @pl.when(i == 2 * lag)
        def _():
            vocab_copy.wait()
            for k in range(1, nz):
                zk = me.behind(k)
                remote(
                    target, targets.at[zk], tgt_send.at[k - 1], tgt_recv.at[k - 1], p, me.at(zk)
                ).wait_recv()
            for q in range(nz):
                for j in range(group // lanes):
                    cut = slice(j * lanes, (j + 1) * lanes)
                    ids = [targets[q, k : k + 1, cut] for k in range(topk)]
                    weights = [targets[q, topk + k : topk + k + 1, cut] for k in range(topk)]
                    for k in range(topk):
                        whole = sum(jnp.where(ids[j] == ids[k], weights[j], 0.0) for j in range(topk))
                        columns_of[q, cut, k : k + 1] = rows_to_column(ids[k])
                        columns_of[q, cut, topk + k : topk + k + 1] = rows_to_column(whole)

        @pl.when(i >= 2 * lag)
        def _():
            staged(i - 2 * lag, compute_stage)

        return 0

    lax.fori_loop(0, steps + 2 * lag, gather_step, 0)
    normed_copy = pltpu.make_async_copy(gathered, normed_hbm, out_sem)
    normed_copy.start()

    def plane_stat(kind):
        return remote(stat, stat_plane.at[kind], st_send.at[kind], st_recv.at[kind], me.plane[kind], me.dp)

    for kind in range(3):
        plane_stat(kind).start()

    def combined(mine, others):
        lse = [mine[:nz]] + [o[:nz] for o in others]
        top = functools.reduce(jnp.maximum, lse)
        total = sum(jnp.exp(v - top) for v in lse)
        return top + jnp.log(total), mine[nz:] + sum(o[nz:] for o in others)

    for kind in range(3):
        plane_stat(kind).wait_recv()
    lse, tgt = combined(stat[...], [stat_plane[kind] for kind in range(3)])
    stat_mid[0:nz] = lse
    stat_mid[nz : 2 * nz] = tgt

    def line_stat(k):
        return remote(
            stat_mid, stat_line.at[k - 1], st_send.at[2 + k], st_recv.at[2 + k], p, me.at(me.ahead(k))
        )

    for k in range(1, nz):
        line_stat(k).start()
    for k in range(1, nz):
        line_stat(k).wait_recv()
    lse, tgt = combined(stat_mid[...], [stat_line[k] for k in range(nz - 1)])
    for kind in range(3):
        plane_stat(kind).wait_send()
    stat[0:nz] = lse
    stat[nz : 2 * nz] = tgt
    mine = pl.ds(pl.multiple_of(p * rows, rows), rows)
    own_at = lax.broadcasted_iota(jnp.int32, (2 * nz, rows), 0)
    own_lse = jnp.sum(jnp.where(own_at == z, stat[:, mine], 0.0), axis=0, keepdims=True)
    own_tgt = jnp.sum(jnp.where(own_at == nz + z, stat[:, mine], 0.0), axis=0, keepdims=True)
    losses_out[...] = own_lse - own_tgt + z_weight * own_lse * own_lse

    def grads_copy(q):
        return pltpu.make_async_copy(grads.at[lax.rem(q, 2)], grads_hbm.at[q], grads_sem.at[lax.rem(q, 2)])

    def grads_plane(q, _):
        @pl.when(q >= 2)
        def _():
            grads_copy(q - 2).wait()

        for j in range(group // lanes):
            cut = slice(j * lanes, (j + 1) * lanes)
            lse_col[cut, :] = rows_to_column(row_of(stat, q, cut))

        def some(i, _):
            r = pl.ds(pl.multiple_of(i * chunk, chunk), chunk)
            norm = lse_col[r, :]
            factor = loss_scale * (1.0 + 2.0 * z_weight * norm)
            grads[lax.rem(q, 2), r, :] = (
                jnp.exp(scores[q, r, :] - norm) * factor - loss_scale * wanted_of(q, r)
            ).astype(bf16)
            return 0

        lax.fori_loop(0, group // chunk, some, 0)
        grads_copy(q).start()
        return 0

    lax.fori_loop(0, nz, grads_plane, 0)
    for q in range(max(nz - 2, 0), nz):
        grads_copy(q).wait()
    normed_copy.wait()

    for k in range(1, nz):
        target_copy(k).wait_send()
        line_stat(k).wait_send()
    for t in range(tiles):
        for kind in range(3):
            piece(kind, t).wait_send()
    for zz in range(nz):
        to_x(zz).wait_send()
        to_y(zz).wait_send()
        corner_y(zz).wait_send()

        @pl.when((zz <= z) & (z + 1 < nz))
        def _():
            up(zz).wait_send()

        @pl.when((zz >= z) & (z > 0))
        def _():
            below(zz).wait_send()


def backward_kernel(
    nz,
    normed_hbm,
    grads_hbm,
    vocab_hbm,
    stream,
    final_gain,
    vgrad_hbm,
    sgrad_out,
    normed,
    grads,
    vocab,
    turned,
    block,
    core_send_buf,
    core_recv_buf,
    far_send_buf,
    far_recv_buf,
    part,
    first,
    second,
    line_recv_buf,
    in_sem,
    core_send,
    core_recv,
    far_send,
    far_recv,
    hop_send,
    hop_recv,
    line_send,
    line_recv,
    out_sem,
):
    me = Place(nz)
    p, z, c = me.p, me.z, me.c
    rows, width = stream.shape
    group = grads.shape[1]
    tokens = nz * group
    span = vocab.shape[1]
    deep = width // (nz * CORES)

    ahead = sorted(range(1, nz), key=lambda k: abs(2 * k - nz)) + [nz]

    def normed_load(i, mine):
        side = me.c if mine else 1 - me.c
        at = pl.ds(pl.multiple_of((me.ahead(ahead[i]) * CORES + side) * deep, deep), deep)
        return pltpu.make_async_copy(normed_hbm.at[:, :, at], normed.at[:, :, at], in_sem.at[2 + 2 * i + mine])

    grads_load = pltpu.make_async_copy(grads_hbm, grads, in_sem.at[0])
    vocab_load = pltpu.make_async_copy(
        vocab_hbm.at[:, pl.ds(pl.multiple_of(z * span, span), span)], vocab, in_sem.at[1]
    )
    grads_load.start()
    normed_load(0, 0).start()
    normed_load(0, 1).start()
    vocab_load.start()
    for i in range(1, nz):
        normed_load(i, 0).start()
        normed_load(i, 1).start()

    partner = me.dp + 1 - 2 * c
    greet(
        [(p, partner), (me.px, me.dp), (me.py, me.dp)] + [(p, me.at(me.ahead(k))) for k in range(1, nz)]
    )
    grads_load.wait()

    def core_copy(i):
        return remote(
            core_send_buf.at[i % 2], core_recv_buf.at[i], core_send.at[i], core_recv.at[i], p, partner
        )

    def far_copy(k, zk):
        return remote(
            far_send_buf.at[k - 1], far_recv_buf.at[z], far_send.at[k - 1], far_recv.at[k - 1], p, me.at(zk)
        )

    def product(dest, store):
        at = pl.ds(pl.multiple_of(dest * deep, deep), deep)
        for q in range(nz):
            turned[:, q * group : (q + 1) * group] = normed[q, :, at].T

        def tile(t, _):
            cut = pl.ds(pl.multiple_of(t * TILE, TILE), TILE)
            store(
                cut,
                jnp.dot(
                    turned[...], grads[:, :, cut].reshape(tokens, TILE), preferred_element_type=f32
                ),
            )
            return 0

        lax.fori_loop(0, span // TILE, tile, 0)

    def vocab_step(i):
        k = ahead[i]
        zk = me.ahead(k)
        if i >= 2:
            core_copy(i - 2).wait_send()

        def to_core(cut, value):
            core_send_buf[i % 2, :, cut] = value.astype(bf16)

        normed_load(i, 0).wait()

        product(zk * CORES + 1 - c, to_core)
        core_copy(i).start()

        def to_block(cut, value):
            block[:, cut] = value

        normed_load(i, 1).wait()

        product(me.at(zk), to_block)
        core_copy(i).wait_recv()

        def add(j, _):
            r = pl.ds(pl.multiple_of(j * 32, 32), 32)
            value = (block[r, :] + core_recv_buf[i, r, :].astype(f32)).astype(bf16)

            if k < nz:
                far_send_buf[k - 1, r, :] = value
            else:
                far_recv_buf[z, r, :] = value
            return 0

        lax.fori_loop(0, deep // 32, add, 0)
        if k < nz:
            far_copy(k, zk).start()

    def at_block(q):
        return pl.ds(pl.multiple_of(q * rows, rows), rows)

    def hop(zz, slot):
        even = not isinstance(zz, int) or zz % 2 == 0
        near, target = (me.px, me.px) if even else (me.py, me.py)
        q = near if slot == 0 else me.pd
        return remote(
            part.at[zz, at_block(q), :],
            first.at[zz, slot],
            hop_send.at[zz, slot],
            hop_recv.at[zz, slot],
            target,
            me.dp,
        )

    def turn(zz):
        even = not isinstance(zz, int) or zz % 2 == 0
        target = me.py if even else me.px
        return remote(part.at[zz, at_block(target), :], second.at[zz], hop_send.at[zz, 2], hop_recv.at[zz, 2], target, me.dp)

    half = z // 2
    inner = z * (LINE - 1 - z) // 2
    beside = z + 1 - 2 * lax.rem(z, 2)

    def far_plane(j):
        return (1 - half) * (LINE - 1) + (2 * half - 1) * j

    def line_far(zz):
        target = beside + inner * (zz - beside)
        return remote(
            part.at[zz, at_block(p), :],
            line_recv_buf.at[zz, 0],
            line_send.at[zz],
            line_recv.at[zz, 0],
            p,
            me.at(target),
        )

    def line_near(zz):
        return remote(
            part.at[zz, at_block(p), :],
            line_recv_buf.at[zz, 1],
            line_send.at[zz],
            line_recv.at[zz, 1],
            p,
            me.at(beside),
        )

    step = 16
    pieces = rows // step

    def matmul_stage(zz):
        def tile(t, _):
            cut = pl.ds(pl.multiple_of(t * TILE, TILE), TILE)
            part[zz, :, cut] = lax.dot_general(
                grads[zz], vocab[cut, :], (((1,), (1,)), ((), ())), preferred_element_type=f32
            ).astype(bf16)
            return 0

        lax.fori_loop(0, width // TILE, tile, 0)
        hop(zz, 1).start()
        hop(zz, 0).start()

    def turn_stage(zz):
        hop(zz, 1).wait_recv()
        q = me.py if zz % 2 == 0 else me.px

        def some(i, _):
            r = pl.ds(pl.multiple_of(i * step, step), step)
            at = pl.ds(pl.multiple_of(q * rows + i * step, step), step)
            part[zz, at, :] = (part[zz, at, :].astype(f32) + first[zz, 1, r, :].astype(f32)).astype(bf16)
            return 0

        lax.fori_loop(0, pieces, some, 0)
        turn(zz).start()

    def plane_sum(zz, i):
        r = pl.ds(pl.multiple_of(i * step, step), step)
        at = pl.ds(pl.multiple_of(p * rows + i * step, step), step)
        return (
            part[zz, at, :].astype(f32) + first[zz, 0, r, :].astype(f32) + second[zz, r, :].astype(f32)
        )

    def store_sum(zz, added):
        def some(i, _):
            r = pl.ds(pl.multiple_of(i * step, step), step)
            at = pl.ds(pl.multiple_of(p * rows + i * step, step), step)
            value = plane_sum(zz, i)
            if added:
                value = value + line_recv_buf[zz, 0, r, :].astype(f32)
            part[zz, at, :] = value.astype(bf16)
            return 0

        lax.fori_loop(0, pieces, some, 0)

    def far_stage(j):
        zz = far_plane(j)
        hop(zz, 0).wait_recv()
        turn(zz).wait_recv()

        @pl.when(inner == 0)
        def _():
            store_sum(zz, False)

        @pl.when(inner == 1)
        def _():
            line_far(zz).wait_recv()
            store_sum(zz, True)

        line_far(zz).start()

    def near_stage():
        hop(beside, 0).wait_recv()
        turn(beside).wait_recv()
        store_sum(beside, False)
        line_near(beside).start()

    def last_stage():
        hop(z, 0).wait_recv()
        turn(z).wait_recv()
        line_far(z).wait_recv()
        line_near(z).wait_recv()

        def some(i, _):
            r = pl.ds(pl.multiple_of(i * step, step), step)
            value = plane_sum(z, i)
            for k in range(2):
                value = value + line_recv_buf[z, k, r, :].astype(f32)
            rows_of = stream[r, :]
            inverse = lax.rsqrt(jnp.mean(rows_of * rows_of, axis=1, keepdims=True) + epsilon)
            upstream = value * final_gain[...]
            sgrad_out[r, :] = inverse * (
                upstream - rows_of * inverse * inverse * jnp.mean(upstream * rows_of, axis=1, keepdims=True)
            )
            return 0

        lax.fori_loop(0, pieces, some, 0)

    order = []
    low, high = 0, nz - 1
    while low <= high:
        order.append(high)
        if low < high:
            order.append(low)
        low, high = low + 1, high - 1
    for i in range(nz):
        vocab_step(i)
        if i == 0:
            vocab_load.wait()
        matmul_stage(order[i])
        if i > 0:
            turn_stage(order[i - 1])
    turn_stage(order[nz - 1])
    far_stage(0)
    far_stage(1)
    near_stage()
    last_stage()

    def out_copy(q):
        return pltpu.make_async_copy(
            far_recv_buf.at[q], vgrad_hbm.at[:, pl.ds(pl.multiple_of(q * span, span), span)], out_sem.at[q]
        )

    out_copy(z).start()
    for k in range(1, nz):
        zk = me.behind(k)
        remote(
            far_send_buf.at[k - 1], far_recv_buf.at[zk], far_send.at[k - 1], far_recv.at[k - 1], p, me.at(zk)
        ).wait_recv()
        out_copy(zk).start()
    for q in range(nz):
        out_copy(q).wait()

    for k in range(1, nz):
        far_copy(k, me.ahead(k)).wait_send()
    for i in range(max(nz - 2, 0), nz):
        core_copy(i).wait_send()
    for zz in range(nz):
        hop(zz, 0).wait_send()
        hop(zz, 1).wait_send()
        turn(zz).wait_send()

        @pl.when(zz != z)
        def _():
            line_near(zz).wait_send()


def vmem():
    return pl.BlockSpec(memory_space=pltpu.VMEM)


def anywhere():
    return pl.BlockSpec(memory_space=pl.ANY)


def fast_shards(
    nz, hidden_act, down_weight, residual, post_gain, final_gain, vocab, vocab_bias, target_ids, target_weights
):
    rows, width = residual.shape
    group, hidden_units = hidden_act.shape
    columns = vocab.shape[1]
    span = columns // nz
    topk = target_ids.shape[1]
    tiles = width // TILE
    deep = width // (nz * CORES)
    dma = pltpu.SemaphoreType.DMA
    target = jnp.concatenate([target_ids.astype(f32), target_weights], axis=1).T
    normed, grads, stream, losses = pl.pallas_call(
        functools.partial(forward_kernel, nz, topk),
        name="forward",
        out_shape=(
            jax.ShapeDtypeStruct((nz, group, width), bf16),
            jax.ShapeDtypeStruct((nz, group, span), bf16),
            jax.ShapeDtypeStruct((rows, width), f32),
            jax.ShapeDtypeStruct((1, rows), f32),
        ),
        in_specs=[vmem(), anywhere(), vmem(), vmem(), vmem(), anywhere(), vmem(), vmem()],
        out_specs=(anywhere(), anywhere(), vmem(), vmem()),
        scratch_shapes=[
            pltpu.VMEM((hidden_units, width), bf16),
            pltpu.VMEM((width, span), bf16),
            pltpu.VMEM((group, TILE), f32),
            pltpu.VMEM((rows, width), f32),
            pltpu.VMEM((group, width), bf16),
            pltpu.VMEM((3, rows, width), bf16),
            pltpu.VMEM((nz, group, width), bf16),
            pltpu.VMEM((nz, group, span), f32),
            pltpu.VMEM((nz, 2 * topk, group), f32),
            pltpu.VMEM((nz, group, 2 * topk), f32),
            pltpu.VMEM((group, 1), f32),
            pltpu.VMEM((group, 1), f32),
            pltpu.VMEM((2 * nz, group), f32),
            pltpu.VMEM((3, 2 * nz, group), f32),
            pltpu.VMEM((2 * nz, group), f32),
            pltpu.VMEM((nz - 1, 2 * nz, group), f32),
            pltpu.VMEM((2, group, span), bf16),
            dma((tiles,)),
            dma,
            dma((nz - 1,)),
            dma((nz - 1,)),
            dma((3, tiles)),
            dma((3, tiles)),
            dma((nz, 5)),
            dma((nz, 4)),
            dma((nz + 2,)),
            dma((nz + 2,)),
            dma,
            dma((2,)),
        ],
        compiler_params=pltpu.CompilerParams(
            collective_id=0, has_side_effects=True, vmem_limit_bytes=66 * 1000 * 1000
        ),
    )(
        hidden_act,
        down_weight,
        residual,
        post_gain[None, :],
        final_gain[None, :],
        vocab,
        vocab_bias[None, :],
        target,
    )
    vocab_grad, stream_grad = pl.pallas_call(
        functools.partial(backward_kernel, nz),
        name="backward",
        out_shape=(
            jax.ShapeDtypeStruct((deep, columns), bf16),
            jax.ShapeDtypeStruct((rows, width), f32),
        ),
        in_specs=[anywhere(), anywhere(), anywhere(), vmem(), vmem()],
        out_specs=(anywhere(), vmem()),
        scratch_shapes=[
            pltpu.VMEM((nz, group, width), bf16),
            pltpu.VMEM((nz, group, span), bf16),
            pltpu.VMEM((width, span), bf16),
            pltpu.VMEM((deep, nz * group), bf16),
            pltpu.VMEM((deep, span), f32),
            pltpu.VMEM((2, deep, span), bf16),
            pltpu.VMEM((nz, deep, span), bf16),
            pltpu.VMEM((nz - 1, deep, span), bf16),
            pltpu.VMEM((nz, deep, span), bf16),
            pltpu.VMEM((nz, group, width), bf16),
            pltpu.VMEM((nz, 2, rows, width), bf16),
            pltpu.VMEM((nz, rows, width), bf16),
            pltpu.VMEM((nz, 2, rows, width), bf16),
            dma((2 + 2 * nz,)),
            dma((nz,)),
            dma((nz,)),
            dma((nz - 1,)),
            dma((nz - 1,)),
            dma((nz, 3)),
            dma((nz, 3)),
            dma((nz,)),
            dma((nz, 2)),
            dma((nz,)),
        ],
        compiler_params=pltpu.CompilerParams(
            collective_id=1, has_side_effects=True, vmem_limit_bytes=66 * 1000 * 1000
        ),
    )(normed, grads, vocab, stream, final_gain[None, :])
    return losses[0], stream_grad, vocab_grad.astype(f32)


def inverse_rms(values):
    return lax.rsqrt(jnp.mean(values * values, axis=-1, keepdims=True) + epsilon)


def general_shards(
    hidden_act,
    down_weight,
    residual,
    post_gain,
    final_gain,
    vocab,
    vocab_bias,
    target_ids,
    target_weights,
):
    own_rows = residual.shape[0]
    group_rows = hidden_act.shape[0]
    columns = vocab.shape[1]
    vp_index = lax.axis_index("vp")
    branch = lax.psum_scatter(
        jnp.dot(hidden_act, down_weight, preferred_element_type=jnp.float32),
        "vp",
        scatter_dimension=0,
        tiled=True,
    )
    stream = residual.astype(jnp.float32) + branch * inverse_rms(branch) * post_gain
    inverse = inverse_rms(stream)
    normed = (stream * inverse * final_gain).astype(jnp.bfloat16)
    gathered = lax.all_gather(normed, "vp", axis=0, tiled=True)
    local_ids = target_ids - vp_index * columns
    position = lax.broadcasted_iota(jnp.int32, (1, columns), 1)
    wanted = jnp.zeros((group_rows, columns), jnp.float32)
    for target_k in range(target_ids.shape[1]):
        wanted = wanted + jnp.where(
            local_ids[:, target_k : target_k + 1] == position,
            target_weights[:, target_k : target_k + 1],
            0.0,
        )
    scores = jnp.dot(gathered, vocab, preferred_element_type=jnp.float32) + vocab_bias[None, :]
    local_max = jnp.max(scores, axis=1)
    local_sum = jnp.sum(jnp.exp(scores - local_max[:, None]), axis=1)
    local_target = jnp.sum(wanted * scores, axis=1)
    stats = lax.all_gather(jnp.stack([local_max, local_sum, local_target]), "vp", axis=0)
    row_max = jnp.max(stats[:, 0], axis=0)
    row_sum = jnp.sum(stats[:, 1] * jnp.exp(stats[:, 0] - row_max), axis=0)
    target_score = jnp.sum(stats[:, 2], axis=0)
    log_norm = row_max + jnp.log(row_sum)
    group_losses = log_norm - target_score + z_weight * log_norm * log_norm
    losses = lax.dynamic_slice_in_dim(group_losses, vp_index * own_rows, own_rows, 0)
    factor = (1.0 + 2.0 * z_weight * log_norm)[:, None]
    probability = jnp.exp(scores - log_norm[:, None])
    score_grads = (loss_scale * (probability * factor - wanted)).astype(jnp.bfloat16)
    chunk = columns // CHUNKS
    pieces = []
    for index in range(CHUNKS):
        part = score_grads[:, index * chunk : (index + 1) * chunk]
        grad = lax.dot_general(
            gathered, part, (((0,), (0,)), ((), ())), preferred_element_type=jnp.float32
        ).astype(jnp.bfloat16)
        pieces.append(lax.psum_scatter(grad, "dp", scatter_dimension=0, tiled=True))
    row_grad = lax.psum_scatter(
        lax.dot_general(
            score_grads, vocab, (((1,), (1,)), ((), ())), preferred_element_type=jnp.float32
        ),
        "vp",
        scatter_dimension=0,
        tiled=True,
    )
    vocab_grad = jnp.concatenate([piece.astype(jnp.float32) for piece in pieces], axis=1)
    upstream = row_grad * final_gain
    stream_grad = inverse * (
        upstream - stream * inverse * inverse * jnp.mean(upstream * stream, axis=-1, keepdims=True)
    )
    return (losses, stream_grad, vocab_grad)


def solution(mesh):
    in_specs = (
        P("dp", "vp"),
        P("vp", None),
        P(("dp", "vp"), None),
        P(),
        P(),
        P(None, "vp"),
        P("vp"),
        P("dp", None),
        P("dp", None),
    )
    out_specs = (P(("dp", "vp")), P(("dp", "vp"), None), P("dp", "vp"))
    body = general_shards
    if mesh.shape["vp"] == PLANE and mesh.shape["dp"] == LINE * CORES:
        body = functools.partial(fast_shards, LINE)
    return jax.shard_map(body, mesh=mesh, in_specs=in_specs, out_specs=out_specs, check_vma=False)
```

```python
import functools

import jax
import jax.numpy as jnp
from jax import lax
from jax.experimental import pallas as pl
from jax.experimental.pallas import tpu as pltpu
from jax.sharding import PartitionSpec as P

MESH = pl.DeviceIdType.MESH
CORES = 2
PLANE = 4
LINE = 4
TILE = 1024
CHUNKS = 4

epsilon = 1e-06
z_weight = 0.001
loss_scale = 32.0
f32 = jnp.float32
bf16 = jnp.bfloat16


def remote(src, dst, send_sem, recv_sem, vp, dp):
    return pltpu.make_async_remote_copy(
        src_ref=src,
        dst_ref=dst,
        send_sem=send_sem,
        recv_sem=recv_sem,
        device_id={"vp": vp, "dp": dp},
        device_id_type=MESH,
    )


class Place:
    def __init__(self, nz):
        self.nz = nz
        self.p = lax.axis_index("vp")
        self.dp = lax.axis_index("dp")
        self.z = self.dp // CORES
        self.c = lax.rem(self.dp, CORES)
        self.px = self.p + 1 - 2 * lax.rem(self.p, 2)
        self.py = lax.rem(self.p + 2, PLANE)
        self.pd = PLANE - 1 - self.p
        self.plane = (self.px, self.py, self.pd)

    def at(self, z):
        return z * CORES + self.c

    def ahead(self, k):
        return lax.rem(self.z + k, self.nz)

    def behind(self, k):
        return lax.rem(self.z - k + self.nz, self.nz)


def greet(peers):
    barrier = pltpu.get_barrier_semaphore()
    for vp, dp in peers:
        pl.semaphore_signal(barrier, inc=1, device_id={"vp": vp, "dp": dp}, device_id_type=MESH)
    pl.semaphore_wait(barrier, len(peers))


def rows_to_column(row):
    n = row.shape[1]
    eye = lax.broadcasted_iota(jnp.int32, (n, n), 0) == lax.broadcasted_iota(jnp.int32, (n, n), 1)
    return jnp.sum(jnp.where(eye, row, 0.0), axis=1, keepdims=True)


def column_to_row(column):
    n = column.shape[0]
    eye = lax.broadcasted_iota(jnp.int32, (n, n), 0) == lax.broadcasted_iota(jnp.int32, (n, n), 1)
    return jnp.sum(jnp.where(eye, column, 0.0), axis=0, keepdims=True)


def forward_kernel(
    nz,
    topk,
    hidden,
    down_hbm,
    resid,
    post_gain,
    final_gain,
    vocab_hbm,
    bias,
    target,
    normed_hbm,
    grads_hbm,
    stream_out,
    losses_out,
    down,
    vocab,
    partial,
    own,
    tosend,
    arrived,
    gathered,
    scores,
    targets,
    columns_of,
    lse_col,
    tgt_col,
    stat,
    stat_plane,
    stat_mid,
    stat_line,
    grads,
    down_sem,
    vocab_sem,
    tgt_send,
    tgt_recv,
    rs_send,
    rs_recv,
    ag_send,
    ag_recv,
    st_send,
    st_recv,
    out_sem,
    grads_sem,
):
    me = Place(nz)
    p, z, c = me.p, me.z, me.c
    rows, width = resid.shape
    group = hidden.shape[0]
    span = vocab.shape[1]
    tiles = width // TILE
    lanes = 128

    def down_copy(t):
        cut = pl.ds(pl.multiple_of(t * TILE, TILE), TILE)
        return pltpu.make_async_copy(down_hbm.at[:, cut], down.at[:, cut], down_sem.at[t])

    for t in range(tiles):
        down_copy(t).start()
    vocab_copy = pltpu.make_async_copy(
        vocab_hbm.at[:, pl.ds(pl.multiple_of(z * span, span), span)], vocab, vocab_sem
    )
    vocab_copy.start()

    line = [(p, me.at(me.ahead(k))) for k in range(1, nz)]
    greet([(q, me.dp) for q in me.plane] + line)

    def target_copy(k):
        return remote(target, targets.at[z], tgt_send.at[k - 1], tgt_recv.at[k - 1], p, me.at(me.ahead(k)))

    for k in range(1, nz):
        target_copy(k).start()
    targets[z] = target[...]

    def piece(kind, t):
        q = me.plane[kind]
        cut = pl.ds(pl.multiple_of(t * TILE, TILE), TILE)
        return remote(
            tosend.at[pl.ds(pl.multiple_of(q * rows, rows), rows), cut],
            arrived.at[kind, :, cut],
            rs_send.at[kind, t],
            rs_recv.at[kind, t],
            q,
            me.dp,
        )

    def down_tile(t, _):
        down_copy(t).wait()
        cut = pl.ds(pl.multiple_of(t * TILE, TILE), TILE)
        partial[...] = jnp.dot(hidden[...], down[:, cut], preferred_element_type=f32)
        tosend[:, cut] = partial[...].astype(bf16)
        own[:, cut] = partial[pl.ds(pl.multiple_of(p * rows, rows), rows), :]
        for kind in (2, 0, 1):
            piece(kind, t).start()
        return 0

    lax.fori_loop(0, tiles, down_tile, 0)

    for k in range(1, nz):
        zk = me.behind(k)
        remote(
            target, targets.at[zk], tgt_send.at[k - 1], tgt_recv.at[k - 1], p, me.at(zk)
        ).wait_recv()
    for q in range(nz):
        for j in range(group // lanes):
            cut = slice(j * lanes, (j + 1) * lanes)
            ids = [targets[q, k : k + 1, cut] for k in range(topk)]
            weights = [targets[q, topk + k : topk + k + 1, cut] for k in range(topk)]
            for k in range(topk):
                whole = sum(jnp.where(ids[j] == ids[k], weights[j], 0.0) for j in range(topk))
                columns_of[q, cut, k : k + 1] = rows_to_column(ids[k])
                columns_of[q, cut, topk + k : topk + k + 1] = rows_to_column(whole)

    for t in range(tiles):
        for kind in range(3):
            piece(kind, t).wait_recv()

    step = 64

    def norm_rows(i, _):
        r = pl.ds(pl.multiple_of(i * step, step), step)
        branch = own[r, :]
        for kind in range(3):
            branch = branch + arrived[kind, r, :].astype(f32)
        scale = lax.rsqrt(jnp.mean(branch * branch, axis=1, keepdims=True) + epsilon)
        stream = resid[r, :].astype(f32) + branch * scale * post_gain[...]
        inverse = lax.rsqrt(jnp.mean(stream * stream, axis=1, keepdims=True) + epsilon)
        stream_out[r, :] = stream
        gathered[z, pl.ds(pl.multiple_of(p * rows + i * step, step), step), :] = (
            stream * inverse * final_gain[...]
        ).astype(bf16)
        return 0

    lax.fori_loop(0, rows // step, norm_rows, 0)

    def block(zz, q):
        return gathered.at[zz, pl.ds(pl.multiple_of(q * rows, rows), rows), :]

    def send(zz, q, way, kind, vp, dp):
        return remote(block(zz, q), block(zz, q), ag_send.at[zz, way], ag_recv.at[zz, kind], vp, dp)

    def to_x(zz):
        return send(zz, p, 0, 1, me.px, me.dp)

    def to_y(zz):
        return send(zz, p, 1, 2, me.py, me.dp)

    def up(zz):
        return send(zz, p, 2, 0, p, me.dp + CORES)

    def below(zz):
        return send(zz, p, 3, 0, p, me.dp - CORES)

    def corner_y(zz):
        return send(zz, me.px, 4, 3, me.py, me.dp)

    def corner_x(zz):
        return send(zz, me.py, 4, 3, me.px, me.dp)

    def landed(zz, kind, q):
        return remote(block(zz, q), block(zz, q), ag_send.at[zz, 0], ag_recv.at[zz, kind], p, me.dp)

    def column_stage(s, zz):
        @pl.when(s > 0)
        def _():
            landed(zz, 0, p).wait_recv()

        @pl.when((zz <= z) & (z + 1 < nz))
        def _():
            up(zz).start()

        @pl.when((zz >= z) & (z > 0))
        def _():
            below(zz).start()

        to_x(zz).start()
        to_y(zz).start()

    def corner_stage(zz):
        landed(zz, 1, me.px).wait_recv()

        @pl.when(lax.rem(zz, 2) == 0)
        def _():
            corner_y(zz).start()

        landed(zz, 2, me.py).wait_recv()

        @pl.when(lax.rem(zz, 2) == 1)
        def _():
            corner_x(zz).start()

    first_column = p * vocab_hbm.shape[1] + z * span
    position = lax.broadcasted_iota(jnp.int32, (1, span), 1).astype(f32)
    chunk = 128

    def wanted_of(zz, r):
        total = 0.0
        for k in range(topk):
            ids = columns_of[zz, r, k : k + 1] - first_column.astype(f32)
            total = jnp.where(ids == position, columns_of[zz, r, topk + k : topk + k + 1], total)
        return total

    row_at = lax.broadcasted_iota(jnp.int32, (2 * nz, lanes), 0)
    stat[...] = jnp.zeros_like(stat)

    def row_of(ref, q, cut):
        return jnp.sum(jnp.where(row_at == q, ref[:, cut], 0.0), axis=0, keepdims=True)

    pair = 2 * rows

    def compute_pair(zz, which):
        base = which * pair

        def tile(t, _):
            cut = pl.ds(pl.multiple_of(t * TILE, TILE), TILE)
            at = pl.ds(pl.multiple_of(z * span + t * TILE, TILE), TILE)
            r = pl.ds(pl.multiple_of(base, pair), pair)
            scores[zz, r, cut] = (
                jnp.dot(gathered[zz, r, :], vocab[:, cut], preferred_element_type=f32) + bias[:, at]
            )
            return 0

        lax.fori_loop(0, span // TILE, tile, 0)

        def stats(i, _):
            r = pl.ds(pl.multiple_of(base + i * chunk, chunk), chunk)
            at = pl.ds(pl.multiple_of(i * chunk, chunk), chunk)
            values = scores[zz, r, :]
            largest = jnp.max(values, axis=1, keepdims=True)
            total = jnp.sum(jnp.exp(values - largest), axis=1, keepdims=True)
            lse_col[at, :] = largest + jnp.log(total)
            tgt_col[at, :] = jnp.sum(wanted_of(zz, r) * values, axis=1, keepdims=True)
            return 0

        lax.fori_loop(0, pair // chunk, stats, 0)
        for j in range(pair // lanes):
            cut = slice(j * lanes, (j + 1) * lanes)
            at = pl.ds(pl.multiple_of(base + j * lanes, lanes), lanes)
            kept = jnp.where(row_at == zz, column_to_row(lse_col[cut, :]), stat[:, at])
            stat[:, at] = jnp.where(row_at == nz + zz, column_to_row(tgt_col[cut, :]), kept)

    def compute_stage(zz):
        compute_pair(zz, p // 2)
        landed(zz, 3, me.pd).wait_recv()
        compute_pair(zz, 1 - p // 2)

    steps = 2 * nz - 1
    lag = 2

    def gather_step(i, _):
        def staged(s, stage):
            half = (s + 1) // 2
            zz = z + half * (1 - 2 * lax.rem(s, 2))

            @pl.when((zz >= 0) & (zz < nz))
            def _():
                stage(zz)

        @pl.when(i < steps)
        def _():
            staged(i, functools.partial(column_stage, i))

        @pl.when((i >= lag) & (i < steps + lag))
        def _():
            staged(i - lag, corner_stage)

        @pl.when(i == 2 * lag)
        def _():
            vocab_copy.wait()

        @pl.when(i >= 2 * lag)
        def _():
            staged(i - 2 * lag, compute_stage)

        return 0

    lax.fori_loop(0, steps + 2 * lag, gather_step, 0)
    normed_copy = pltpu.make_async_copy(gathered, normed_hbm, out_sem)
    normed_copy.start()

    def plane_stat(kind):
        return remote(stat, stat_plane.at[kind], st_send.at[kind], st_recv.at[kind], me.plane[kind], me.dp)

    for kind in range(3):
        plane_stat(kind).start()

    def combined(mine, others):
        lse = [mine[:nz]] + [o[:nz] for o in others]
        top = functools.reduce(jnp.maximum, lse)
        total = sum(jnp.exp(v - top) for v in lse)
        return top + jnp.log(total), mine[nz:] + sum(o[nz:] for o in others)

    for kind in range(3):
        plane_stat(kind).wait_recv()
    lse, tgt = combined(stat[...], [stat_plane[kind] for kind in range(3)])
    stat_mid[0:nz] = lse
    stat_mid[nz : 2 * nz] = tgt

    def line_stat(k):
        return remote(
            stat_mid, stat_line.at[k - 1], st_send.at[2 + k], st_recv.at[2 + k], p, me.at(me.ahead(k))
        )

    for k in range(1, nz):
        line_stat(k).start()
    for k in range(1, nz):
        line_stat(k).wait_recv()
    lse, tgt = combined(stat_mid[...], [stat_line[k] for k in range(nz - 1)])
    for kind in range(3):
        plane_stat(kind).wait_send()
    stat[0:nz] = lse
    stat[nz : 2 * nz] = tgt
    mine = pl.ds(pl.multiple_of(p * rows, rows), rows)
    own_at = lax.broadcasted_iota(jnp.int32, (2 * nz, rows), 0)
    own_lse = jnp.sum(jnp.where(own_at == z, stat[:, mine], 0.0), axis=0, keepdims=True)
    own_tgt = jnp.sum(jnp.where(own_at == nz + z, stat[:, mine], 0.0), axis=0, keepdims=True)
    losses_out[...] = own_lse - own_tgt + z_weight * own_lse * own_lse

    def grads_copy(q):
        return pltpu.make_async_copy(grads.at[lax.rem(q, 2)], grads_hbm.at[q], grads_sem.at[lax.rem(q, 2)])

    def grads_plane(q, _):
        @pl.when(q >= 2)
        def _():
            grads_copy(q - 2).wait()

        for j in range(group // lanes):
            cut = slice(j * lanes, (j + 1) * lanes)
            lse_col[cut, :] = rows_to_column(row_of(stat, q, cut))

        def some(i, _):
            r = pl.ds(pl.multiple_of(i * chunk, chunk), chunk)
            norm = lse_col[r, :]
            factor = loss_scale * (1.0 + 2.0 * z_weight * norm)
            grads[lax.rem(q, 2), r, :] = (
                jnp.exp(scores[q, r, :] - norm) * factor - loss_scale * wanted_of(q, r)
            ).astype(bf16)
            return 0

        lax.fori_loop(0, group // chunk, some, 0)
        grads_copy(q).start()
        return 0

    lax.fori_loop(0, nz, grads_plane, 0)
    for q in range(max(nz - 2, 0), nz):
        grads_copy(q).wait()
    normed_copy.wait()

    for k in range(1, nz):
        target_copy(k).wait_send()
        line_stat(k).wait_send()
    for t in range(tiles):
        for kind in range(3):
            piece(kind, t).wait_send()
    for zz in range(nz):
        to_x(zz).wait_send()
        to_y(zz).wait_send()
        corner_y(zz).wait_send()

        @pl.when((zz <= z) & (z + 1 < nz))
        def _():
            up(zz).wait_send()

        @pl.when((zz >= z) & (z > 0))
        def _():
            below(zz).wait_send()


def backward_kernel(
    nz,
    normed_hbm,
    grads_hbm,
    vocab_hbm,
    stream,
    final_gain,
    vgrad_hbm,
    sgrad_out,
    normed,
    grads,
    vocab,
    turned,
    block,
    core_send_buf,
    core_recv_buf,
    far_send_buf,
    far_recv_buf,
    part,
    first,
    second,
    line_recv_buf,
    in_sem,
    core_send,
    core_recv,
    far_send,
    far_recv,
    hop_send,
    hop_recv,
    line_send,
    line_recv,
    out_sem,
):
    me = Place(nz)
    p, z, c = me.p, me.z, me.c
    rows, width = stream.shape
    group = grads.shape[1]
    tokens = nz * group
    span = vocab.shape[1]
    deep = width // (nz * CORES)

    ahead = sorted(range(1, nz), key=lambda k: abs(2 * k - nz)) + [nz]

    def normed_load(i, mine):
        side = me.c if mine else 1 - me.c
        at = pl.ds(pl.multiple_of((me.ahead(ahead[i]) * CORES + side) * deep, deep), deep)
        return pltpu.make_async_copy(normed_hbm.at[:, :, at], normed.at[:, :, at], in_sem.at[2 + 2 * i + mine])

    grads_load = pltpu.make_async_copy(grads_hbm, grads, in_sem.at[0])
    vocab_load = pltpu.make_async_copy(
        vocab_hbm.at[:, pl.ds(pl.multiple_of(z * span, span), span)], vocab, in_sem.at[1]
    )
    grads_load.start()
    normed_load(0, 0).start()
    normed_load(0, 1).start()
    vocab_load.start()
    for i in range(1, nz):
        normed_load(i, 0).start()
        normed_load(i, 1).start()

    partner = me.dp + 1 - 2 * c
    greet(
        [(p, partner), (me.px, me.dp), (me.py, me.dp)] + [(p, me.at(me.ahead(k))) for k in range(1, nz)]
    )
    grads_load.wait()

    def core_copy(i):
        return remote(
            core_send_buf.at[i % 2], core_recv_buf.at[i], core_send.at[i], core_recv.at[i], p, partner
        )

    def far_copy(k, zk):
        return remote(
            far_send_buf.at[k - 1], far_recv_buf.at[z], far_send.at[k - 1], far_recv.at[k - 1], p, me.at(zk)
        )

    def product(dest, store):
        at = pl.ds(pl.multiple_of(dest * deep, deep), deep)
        for q in range(nz):
            turned[:, q * group : (q + 1) * group] = normed[q, :, at].T

        def tile(t, _):
            cut = pl.ds(pl.multiple_of(t * TILE, TILE), TILE)
            store(
                cut,
                jnp.dot(
                    turned[...], grads[:, :, cut].reshape(tokens, TILE), preferred_element_type=f32
                ),
            )
            return 0

        lax.fori_loop(0, span // TILE, tile, 0)

    def vocab_step(i):
        k = ahead[i]
        zk = me.ahead(k)
        if i >= 2:
            core_copy(i - 2).wait_send()

        def to_core(cut, value):
            core_send_buf[i % 2, :, cut] = value.astype(bf16)

        normed_load(i, 0).wait()

        product(zk * CORES + 1 - c, to_core)
        core_copy(i).start()

        def to_block(cut, value):
            block[:, cut] = value

        normed_load(i, 1).wait()

        product(me.at(zk), to_block)
        core_copy(i).wait_recv()

        def add(j, _):
            r = pl.ds(pl.multiple_of(j * 128, 128), 128)
            value = (block[r, :] + core_recv_buf[i, r, :].astype(f32)).astype(bf16)

            if k < nz:
                far_send_buf[k - 1, r, :] = value
            else:
                far_recv_buf[z, r, :] = value
            return 0

        lax.fori_loop(0, deep // 128, add, 0)
        if k < nz:
            far_copy(k, zk).start()

    def at_block(q):
        return pl.ds(pl.multiple_of(q * rows, rows), rows)

    def hop(zz, slot):
        even = not isinstance(zz, int) or zz % 2 == 0
        near, target = (me.px, me.px) if even else (me.py, me.py)
        q = near if slot == 0 else me.pd
        return remote(
            part.at[zz, at_block(q), :],
            first.at[zz, slot],
            hop_send.at[zz, slot],
            hop_recv.at[zz, slot],
            target,
            me.dp,
        )

    def turn(zz):
        even = not isinstance(zz, int) or zz % 2 == 0
        target = me.py if even else me.px
        return remote(part.at[zz, at_block(target), :], second.at[zz], hop_send.at[zz, 2], hop_recv.at[zz, 2], target, me.dp)

    half = z // 2
    inner = z * (LINE - 1 - z) // 2
    beside = z + 1 - 2 * lax.rem(z, 2)

    def far_plane(j):
        return (1 - half) * (LINE - 1) + (2 * half - 1) * j

    def line_far(zz):
        target = beside + inner * (zz - beside)
        return remote(
            part.at[zz, at_block(p), :],
            line_recv_buf.at[zz, 0],
            line_send.at[zz],
            line_recv.at[zz, 0],
            p,
            me.at(target),
        )

    def line_near(zz):
        return remote(
            part.at[zz, at_block(p), :],
            line_recv_buf.at[zz, 1],
            line_send.at[zz],
            line_recv.at[zz, 1],
            p,
            me.at(beside),
        )

    step = 64
    pieces = rows // step

    def matmul_stage(zz):
        def tile(t, _):
            cut = pl.ds(pl.multiple_of(t * TILE, TILE), TILE)
            part[zz, :, cut] = lax.dot_general(
                grads[zz], vocab[cut, :], (((1,), (1,)), ((), ())), preferred_element_type=f32
            ).astype(bf16)
            return 0

        lax.fori_loop(0, width // TILE, tile, 0)
        hop(zz, 1).start()
        hop(zz, 0).start()

    def turn_stage(zz):
        hop(zz, 1).wait_recv()
        q = me.py if zz % 2 == 0 else me.px

        def some(i, _):
            r = pl.ds(pl.multiple_of(i * step, step), step)
            at = pl.ds(pl.multiple_of(q * rows + i * step, step), step)
            part[zz, at, :] = (part[zz, at, :].astype(f32) + first[zz, 1, r, :].astype(f32)).astype(bf16)
            return 0

        lax.fori_loop(0, pieces, some, 0)
        turn(zz).start()

    def plane_sum(zz, i):
        r = pl.ds(pl.multiple_of(i * step, step), step)
        at = pl.ds(pl.multiple_of(p * rows + i * step, step), step)
        return (
            part[zz, at, :].astype(f32) + first[zz, 0, r, :].astype(f32) + second[zz, r, :].astype(f32)
        )

    def store_sum(zz, added):
        def some(i, _):
            r = pl.ds(pl.multiple_of(i * step, step), step)
            at = pl.ds(pl.multiple_of(p * rows + i * step, step), step)
            value = plane_sum(zz, i)
            if added:
                value = value + line_recv_buf[zz, 0, r, :].astype(f32)
            part[zz, at, :] = value.astype(bf16)
            return 0

        lax.fori_loop(0, pieces, some, 0)

    def far_stage(j):
        zz = far_plane(j)
        hop(zz, 0).wait_recv()
        turn(zz).wait_recv()

        @pl.when(inner == 0)
        def _():
            store_sum(zz, False)

        @pl.when(inner == 1)
        def _():
            line_far(zz).wait_recv()
            store_sum(zz, True)

        line_far(zz).start()

    def near_stage():
        hop(beside, 0).wait_recv()
        turn(beside).wait_recv()
        store_sum(beside, False)
        line_near(beside).start()

    def last_stage():
        hop(z, 0).wait_recv()
        turn(z).wait_recv()
        line_far(z).wait_recv()
        line_near(z).wait_recv()

        def some(i, _):
            r = pl.ds(pl.multiple_of(i * step, step), step)
            value = plane_sum(z, i)
            for k in range(2):
                value = value + line_recv_buf[z, k, r, :].astype(f32)
            rows_of = stream[r, :]
            inverse = lax.rsqrt(jnp.mean(rows_of * rows_of, axis=1, keepdims=True) + epsilon)
            upstream = value * final_gain[...]
            sgrad_out[r, :] = inverse * (
                upstream - rows_of * inverse * inverse * jnp.mean(upstream * rows_of, axis=1, keepdims=True)
            )
            return 0

        lax.fori_loop(0, pieces, some, 0)

    order = []
    low, high = 0, nz - 1
    while low <= high:
        order.append(high)
        if low < high:
            order.append(low)
        low, high = low + 1, high - 1
    for i in range(nz):
        vocab_step(i)
        if i == 0:
            vocab_load.wait()
        matmul_stage(order[i])
        if i > 0:
            turn_stage(order[i - 1])
    turn_stage(order[nz - 1])
    far_stage(0)
    far_stage(1)
    near_stage()
    last_stage()

    def out_copy(q):
        return pltpu.make_async_copy(
            far_recv_buf.at[q], vgrad_hbm.at[:, pl.ds(pl.multiple_of(q * span, span), span)], out_sem.at[q]
        )

    out_copy(z).start()
    for k in range(1, nz):
        zk = me.behind(k)
        remote(
            far_send_buf.at[k - 1], far_recv_buf.at[zk], far_send.at[k - 1], far_recv.at[k - 1], p, me.at(zk)
        ).wait_recv()
        out_copy(zk).start()
    for q in range(nz):
        out_copy(q).wait()

    for k in range(1, nz):
        far_copy(k, me.ahead(k)).wait_send()
    for i in range(max(nz - 2, 0), nz):
        core_copy(i).wait_send()
    for zz in range(nz):
        hop(zz, 0).wait_send()
        hop(zz, 1).wait_send()
        turn(zz).wait_send()

        @pl.when(zz != z)
        def _():
            line_near(zz).wait_send()


def vmem():
    return pl.BlockSpec(memory_space=pltpu.VMEM)


def anywhere():
    return pl.BlockSpec(memory_space=pl.ANY)


def fast_shards(
    nz, hidden_act, down_weight, residual, post_gain, final_gain, vocab, vocab_bias, target_ids, target_weights
):
    rows, width = residual.shape
    group, hidden_units = hidden_act.shape
    columns = vocab.shape[1]
    span = columns // nz
    topk = target_ids.shape[1]
    tiles = width // TILE
    deep = width // (nz * CORES)
    if width % TILE or span % TILE or deep % 128 or rows % 128 or group != PLANE * rows:
        return general_shards(
            hidden_act,
            down_weight,
            residual,
            post_gain,
            final_gain,
            vocab,
            vocab_bias,
            target_ids,
            target_weights,
        )
    dma = pltpu.SemaphoreType.DMA
    target = jnp.concatenate([target_ids.astype(f32), target_weights], axis=1).T
    normed, grads, stream, losses = pl.pallas_call(
        functools.partial(forward_kernel, nz, topk),
        name="forward",
        out_shape=(
            jax.ShapeDtypeStruct((nz, group, width), bf16),
            jax.ShapeDtypeStruct((nz, group, span), bf16),
            jax.ShapeDtypeStruct((rows, width), f32),
            jax.ShapeDtypeStruct((1, rows), f32),
        ),
        in_specs=[vmem(), anywhere(), vmem(), vmem(), vmem(), anywhere(), vmem(), vmem()],
        out_specs=(anywhere(), anywhere(), vmem(), vmem()),
        scratch_shapes=[
            pltpu.VMEM((hidden_units, width), bf16),
            pltpu.VMEM((width, span), bf16),
            pltpu.VMEM((group, TILE), f32),
            pltpu.VMEM((rows, width), f32),
            pltpu.VMEM((group, width), bf16),
            pltpu.VMEM((3, rows, width), bf16),
            pltpu.VMEM((nz, group, width), bf16),
            pltpu.VMEM((nz, group, span), f32),
            pltpu.VMEM((nz, 2 * topk, group), f32),
            pltpu.VMEM((nz, group, 2 * topk), f32),
            pltpu.VMEM((group, 1), f32),
            pltpu.VMEM((group, 1), f32),
            pltpu.VMEM((2 * nz, group), f32),
            pltpu.VMEM((3, 2 * nz, group), f32),
            pltpu.VMEM((2 * nz, group), f32),
            pltpu.VMEM((nz - 1, 2 * nz, group), f32),
            pltpu.VMEM((2, group, span), bf16),
            dma((tiles,)),
            dma,
            dma((nz - 1,)),
            dma((nz - 1,)),
            dma((3, tiles)),
            dma((3, tiles)),
            dma((nz, 5)),
            dma((nz, 4)),
            dma((nz + 2,)),
            dma((nz + 2,)),
            dma,
            dma((2,)),
        ],
        compiler_params=pltpu.CompilerParams(
            collective_id=0, has_side_effects=True, vmem_limit_bytes=66 * 1000 * 1000
        ),
    )(
        hidden_act,
        down_weight,
        residual,
        post_gain[None, :],
        final_gain[None, :],
        vocab,
        vocab_bias[None, :],
        target,
    )
    vocab_grad, stream_grad = pl.pallas_call(
        functools.partial(backward_kernel, nz),
        name="backward",
        out_shape=(
            jax.ShapeDtypeStruct((deep, columns), bf16),
            jax.ShapeDtypeStruct((rows, width), f32),
        ),
        in_specs=[anywhere(), anywhere(), anywhere(), vmem(), vmem()],
        out_specs=(anywhere(), vmem()),
        scratch_shapes=[
            pltpu.VMEM((nz, group, width), bf16),
            pltpu.VMEM((nz, group, span), bf16),
            pltpu.VMEM((width, span), bf16),
            pltpu.VMEM((deep, nz * group), bf16),
            pltpu.VMEM((deep, span), f32),
            pltpu.VMEM((2, deep, span), bf16),
            pltpu.VMEM((nz, deep, span), bf16),
            pltpu.VMEM((nz - 1, deep, span), bf16),
            pltpu.VMEM((nz, deep, span), bf16),
            pltpu.VMEM((nz, group, width), bf16),
            pltpu.VMEM((nz, 2, rows, width), bf16),
            pltpu.VMEM((nz, rows, width), bf16),
            pltpu.VMEM((nz, 2, rows, width), bf16),
            dma((2 + 2 * nz,)),
            dma((nz,)),
            dma((nz,)),
            dma((nz - 1,)),
            dma((nz - 1,)),
            dma((nz, 3)),
            dma((nz, 3)),
            dma((nz,)),
            dma((nz, 2)),
            dma((nz,)),
        ],
        compiler_params=pltpu.CompilerParams(
            collective_id=1, has_side_effects=True, vmem_limit_bytes=66 * 1000 * 1000
        ),
    )(normed, grads, vocab, stream, final_gain[None, :])
    return losses[0], stream_grad, vocab_grad.astype(f32)


def inverse_rms(values):
    return lax.rsqrt(jnp.mean(values * values, axis=-1, keepdims=True) + epsilon)


def general_shards(
    hidden_act,
    down_weight,
    residual,
    post_gain,
    final_gain,
    vocab,
    vocab_bias,
    target_ids,
    target_weights,
):
    own_rows = residual.shape[0]
    group_rows = hidden_act.shape[0]
    columns = vocab.shape[1]
    vp_index = lax.axis_index("vp")
    branch = lax.psum_scatter(
        jnp.dot(hidden_act, down_weight, preferred_element_type=jnp.float32),
        "vp",
        scatter_dimension=0,
        tiled=True,
    )
    stream = residual.astype(jnp.float32) + branch * inverse_rms(branch) * post_gain
    inverse = inverse_rms(stream)
    normed = (stream * inverse * final_gain).astype(jnp.bfloat16)
    gathered = lax.all_gather(normed, "vp", axis=0, tiled=True)
    local_ids = target_ids - vp_index * columns
    position = lax.broadcasted_iota(jnp.int32, (1, columns), 1)
    wanted = jnp.zeros((group_rows, columns), jnp.float32)
    for target_k in range(target_ids.shape[1]):
        wanted = wanted + jnp.where(
            local_ids[:, target_k : target_k + 1] == position,
            target_weights[:, target_k : target_k + 1],
            0.0,
        )
    scores = jnp.dot(gathered, vocab, preferred_element_type=jnp.float32) + vocab_bias[None, :]
    local_max = jnp.max(scores, axis=1)
    local_sum = jnp.sum(jnp.exp(scores - local_max[:, None]), axis=1)
    local_target = jnp.sum(wanted * scores, axis=1)
    stats = lax.all_gather(jnp.stack([local_max, local_sum, local_target]), "vp", axis=0)
    row_max = jnp.max(stats[:, 0], axis=0)
    row_sum = jnp.sum(stats[:, 1] * jnp.exp(stats[:, 0] - row_max), axis=0)
    target_score = jnp.sum(stats[:, 2], axis=0)
    log_norm = row_max + jnp.log(row_sum)
    group_losses = log_norm - target_score + z_weight * log_norm * log_norm
    losses = lax.dynamic_slice_in_dim(group_losses, vp_index * own_rows, own_rows, 0)
    factor = (1.0 + 2.0 * z_weight * log_norm)[:, None]
    probability = jnp.exp(scores - log_norm[:, None])
    score_grads = (loss_scale * (probability * factor - wanted)).astype(jnp.bfloat16)
    chunk = columns // CHUNKS
    pieces = []
    for index in range(CHUNKS):
        part = score_grads[:, index * chunk : (index + 1) * chunk]
        grad = lax.dot_general(
            gathered, part, (((0,), (0,)), ((), ())), preferred_element_type=jnp.float32
        ).astype(jnp.bfloat16)
        pieces.append(lax.psum_scatter(grad, "dp", scatter_dimension=0, tiled=True))
    row_grad = lax.psum_scatter(
        lax.dot_general(
            score_grads, vocab, (((1,), (1,)), ((), ())), preferred_element_type=jnp.float32
        ),
        "vp",
        scatter_dimension=0,
        tiled=True,
    )
    vocab_grad = jnp.concatenate([piece.astype(jnp.float32) for piece in pieces], axis=1)
    upstream = row_grad * final_gain
    stream_grad = inverse * (
        upstream - stream * inverse * inverse * jnp.mean(upstream * stream, axis=-1, keepdims=True)
    )
    return (losses, stream_grad, vocab_grad)


def solution(mesh):
    in_specs = (
        P("dp", "vp"),
        P("vp", None),
        P(("dp", "vp"), None),
        P(),
        P(),
        P(None, "vp"),
        P("vp"),
        P("dp", None),
        P("dp", None),
    )
    out_specs = (P(("dp", "vp")), P(("dp", "vp"), None), P("dp", "vp"))
    body = general_shards
    if mesh.shape["vp"] == PLANE and mesh.shape["dp"] == LINE * CORES:
        body = functools.partial(fast_shards, LINE)
    return jax.shard_map(body, mesh=mesh, in_specs=in_specs, out_specs=out_specs, check_vma=False)
```
